32 devices in a mesh: fs: 8 (over z, y), tp: 4 (over x, core).
Axes of the slice: x: 2, y: 2, z: 4, core: 2. Of those that a mesh axis runs over, the one named last changes fastest.
Arguments:
- tokens: bfloat16 [3072, 2048], P(('fs', 'tp')), may hold values from -6 to 6
- ffn1_gain: float32 [2048], replicated, may hold values from 0.1 to 1.9
- ffn1_gate: bfloat16 [2048, 5632], P('fs', 'tp'), may hold values from -0.125 to 0.125
- ffn1_up: bfloat16 [2048, 5632], P('fs', 'tp'), may hold values from -0.125 to 0.125
- ffn1_down: bfloat16 [5632, 2048], P('tp', 'fs'), may hold values from -0.078125 to 0.078125
- mix_gain: float32 [2048], replicated, may hold values from 0.1 to 1.9
- lru_in_weight: bfloat16 [2048, 1536], P('fs', 'tp'), may hold values from -0.125 to 0.125
- lru_gate_weight: bfloat16 [2048, 1536], P('fs', 'tp'), may hold values from -0.125 to 0.125
- conv_weight: bfloat16 [4, 1536], P(None, 'tp'), may hold values from -3 to 3
- gate_a_weight: bfloat16 [24, 64, 64], P('tp'), may hold values from -0.75 to 0.75
- gate_x_weight: bfloat16 [24, 64, 64], P('tp'), may hold values from -0.75 to 0.75
- decay_param: float32 [1536], P('tp'), may hold values from 3.7 to 9
- mix_out_weight: bfloat16 [1536, 2048], P('tp', 'fs'), may hold values from -0.15625 to 0.15625
- ffn2_gain: float32 [2048], replicated, may hold values from 0.1 to 1.9
- ffn2_gate: bfloat16 [2048, 5632], P('fs', 'tp'), may hold values from -0.125 to 0.125
- ffn2_up: bfloat16 [2048, 5632], P('fs', 'tp'), may hold values from -0.125 to 0.125
- ffn2_down: bfloat16 [5632, 2048], P('tp', 'fs'), may hold values from -0.078125 to 0.078125
Outputs:
- layer_out: bfloat16 [3072, 2048], P(('fs', 'tp'))
The draws below stay inside these ranges and needn't reach their ends.
All inputs are finite; a program needn't handle non-finite values.
Results may differ from the reference program's by a relative error of at most 0.017.
Values may be sent and summed in bfloat16 or wider, within the bound.
A program may use at most 64 MiB of HBM per device.

```python
import jax
import jax.numpy as jnp
from jax import lax

D = 2048
FF = 5632
DR = 1536
LB = 64
WIDTH = 4
SEQ = 384
NB = 24
TOKENS = 3072
N_FS = 8
N_TP = 4


def draw_decay_param(key, part):
    first_key, second_key, third_key = jax.random.split(jax.random.fold_in(key, 17), 3)
    slow_share = 0.5
    slow = jax.random.bernoulli(first_key, slow_share, (DR,))
    fast_values = jax.random.uniform(second_key, (DR,), jnp.float32, 3.7, 4.9)
    slow_values = jax.random.uniform(third_key, (DR,), jnp.float32, 7.5, 9.0)
    return jnp.where(slow, slow_values, fast_values).astype(jnp.float32)


def block_scale(own_key, extent, pieces, low, largest):
    loudness = 1.0
    for dim, shards_of in pieces:
        draws = jax.random.uniform(jax.random.fold_in(jax.random.fold_in(own_key, 6), dim), (shards_of,), jnp.float32, low / len(pieces), largest / len(pieces))
        loudness = loudness * jnp.repeat(jnp.exp(draws), extent[dim] // shards_of).reshape((-1,) + (1,) * (len(extent) - 1 - dim))
    return loudness


def normal_values(key, dims, scale, limit, pieces=(), kind=jnp.bfloat16):
    level = block_scale(key, dims, pieces, -0.22, 0.18) if pieces else 1.0
    array = jax.random.normal(key, dims, jnp.float32) * scale * level
    return jnp.minimum(jnp.maximum(array, -limit), limit).astype(kind)


def setup_inputs(seed: int = 0) -> dict:
    key_list = jax.random.split(jax.random.key(seed), 18)
    return {
        "tokens": normal_values(key_list[0], (TOKENS, D), 1.0, 6.0, ((0, 32),)),
        "ffn1_gain": jnp.clip(1.0 + 0.18 * jax.random.normal(key_list[1], (D,), jnp.float32), 0.1, 1.9),
        "ffn1_gate": normal_values(key_list[2], (D, FF), D ** -0.5, 0.125, ((0, 8), (1, 4))),
        "ffn1_up": normal_values(key_list[3], (D, FF), D ** -0.5, 0.125, ((0, 8), (1, 4))),
        "ffn1_down": normal_values(key_list[4], (FF, D), FF ** -0.5, 0.078125, ((0, 4), (1, 8))),
        "mix_gain": jnp.clip(1.0 + 0.18 * jax.random.normal(key_list[5], (D,), jnp.float32), 0.1, 1.9),
        "lru_in_weight": normal_values(key_list[6], (D, DR), D ** -0.5, 0.125, ((0, 8), (1, 4))),
        "lru_gate_weight": normal_values(key_list[7], (D, DR), D ** -0.5, 0.125, ((0, 8), (1, 4))),
        "conv_weight": normal_values(key_list[8], (WIDTH, DR), WIDTH ** -0.5, 3.0, ((1, 4),)),
        "gate_a_weight": normal_values(key_list[9], (NB, LB, LB), LB ** -0.5, 0.75, ((0, 4),)),
        "gate_x_weight": normal_values(key_list[10], (NB, LB, LB), LB ** -0.5, 0.75, ((0, 4),)),
        "decay_param": draw_decay_param(jax.random.fold_in(key_list[17], 71), 0),
        "mix_out_weight": normal_values(key_list[12], (DR, D), DR ** -0.5, 0.15625, ((0, 4), (1, 8))),
        "ffn2_gain": jnp.clip(1.0 + 0.18 * jax.random.normal(key_list[13], (D,), jnp.float32), 0.1, 1.9),
        "ffn2_gate": normal_values(key_list[14], (D, FF), D ** -0.5, 0.125, ((0, 8), (1, 4))),
        "ffn2_up": normal_values(key_list[15], (D, FF), D ** -0.5, 0.125, ((0, 8), (1, 4))),
        "ffn2_down": normal_values(key_list[16], (FF, D), FF ** -0.5, 0.078125, ((0, 4), (1, 8))),
    }


EPS = 1e-06

def rms_rows(values, gain):
    wide = values.astype(jnp.float32)
    scale = lax.rsqrt(lax.optimization_barrier(jnp.mean(wide * wide, axis=-1, keepdims=True)) + EPS)
    return (wide * scale * gain.astype(jnp.float32)).astype(jnp.bfloat16)

def group_sums(hidden, weight):
    rows = hidden.shape[0]
    inner = hidden.shape[1] // N_TP
    hidden_groups = hidden.reshape(rows, N_TP, inner).transpose(1, 0, 2)
    weight_groups = weight.reshape(N_TP, inner, weight.shape[1])

    def add_group(total, pair):
        part = jnp.dot(pair[0], pair[1], preferred_element_type=jnp.float32).astype(jnp.bfloat16)
        return (total + lax.optimization_barrier(part).astype(jnp.float32), None)
    start = jnp.zeros((rows, weight.shape[1]), jnp.float32)
    total, _ = lax.scan(add_group, start, (hidden_groups, weight_groups))
    return total

def half_block(values, gain, gate_weight, up_weight, down_weight):
    normed = rms_rows(values, gain)
    gate = jnp.dot(normed, gate_weight, preferred_element_type=jnp.float32)
    upper = jnp.dot(normed, up_weight, preferred_element_type=jnp.float32)
    hidden = (jax.nn.silu(gate) * upper).astype(jnp.bfloat16)
    return group_sums(hidden, down_weight)

def combine(earlier, later):
    return (earlier[0] * later[0], later[0] * earlier[1] + later[1])

def reference(tokens, ffn1_gain, ffn1_gate, ffn1_up, ffn1_down, mix_gain, lru_in_weight, lru_gate_weight, conv_weight, gate_a_weight, gate_x_weight, decay_param, mix_out_weight, ffn2_gain, ffn2_gate, ffn2_up, ffn2_down):
    first = (tokens.astype(jnp.float32) + 0.5 * half_block(tokens, ffn1_gain, ffn1_gate, ffn1_up, ffn1_down)).astype(jnp.bfloat16)
    normed = rms_rows(first, mix_gain)
    lru_x = jnp.dot(normed, lru_in_weight, preferred_element_type=jnp.float32).astype(jnp.bfloat16)
    lru_gate = jnp.dot(normed, lru_gate_weight, preferred_element_type=jnp.float32).astype(jnp.bfloat16)
    seqs = lru_x.astype(jnp.float32).reshape(N_FS, SEQ, DR)
    padded = jnp.pad(seqs, ((0, 0), (WIDTH - 1, 0), (0, 0)))
    taps = conv_weight.astype(jnp.float32)
    conv = jnp.zeros((N_FS, SEQ, DR), jnp.float32)
    for offset in range(WIDTH):
        conv = conv + taps[offset] * padded[:, WIDTH - 1 - offset:WIDTH - 1 - offset + SEQ]
    conv_low = conv.astype(jnp.bfloat16).astype(jnp.float32)
    blocks = conv_low.reshape(N_FS, SEQ, NB, LB)
    recall = jax.nn.sigmoid(jnp.einsum('nsbi,bij->nsbj', blocks, gate_a_weight.astype(jnp.float32)).reshape(N_FS, SEQ, DR))
    admit = jax.nn.sigmoid(jnp.einsum('nsbi,bij->nsbj', blocks, gate_x_weight.astype(jnp.float32)).reshape(N_FS, SEQ, DR))
    log_keep = -8.0 * recall * jax.nn.softplus(-decay_param)
    drive = jnp.sqrt(-jnp.expm1(2.0 * log_keep)) * admit * conv_low
    _, state = lax.associative_scan(combine, (jnp.exp(log_keep), drive), axis=1)
    mixed = (state.reshape(TOKENS, DR) * jax.nn.gelu(lru_gate.astype(jnp.float32))).astype(jnp.bfloat16)
    second = (first.astype(jnp.float32) + group_sums(mixed, mix_out_weight)).astype(jnp.bfloat16)
    return (second.astype(jnp.float32) + 0.5 * half_block(second, ffn2_gain, ffn2_gate, ffn2_up, ffn2_down)).astype(jnp.bfloat16)
```

```python
import functools
import math

import jax
import jax.numpy as jnp
from jax import lax
from jax.experimental import pallas as pl
from jax.experimental.pallas import tpu as pltpu
from jax.sharding import PartitionSpec as P

EPS = 1e-06
CORES = 2
PAIR = 2
MATS = 3
MESH = pl.DeviceIdType.MESH


def dot_nt(a, b):
    return lax.dot_general(a, b, (((1,), (1,)), ((), ())), preferred_element_type=jnp.float32)


def sigmoid(v):
    return 1.0 / (1.0 + jnp.exp(-v))


def shift_down(values, step, fill):
    pad = jnp.full((step, values.shape[1]), fill, values.dtype)
    return jnp.concatenate([pad, values[: values.shape[0] - step]], axis=0)


class Place:
    def __init__(self, n, t):
        self.n, self.t = n, t
        self.ny = math.isqrt(n // PAIR)
        self.nz = n // self.ny
        self.nq = self.nz // PAIR
        self.nx = t // CORES
        fs, tp = lax.axis_index("fs"), lax.axis_index("tp")
        self.fs, self.tp = fs, tp
        self.z, self.y = fs // self.ny, fs % self.ny
        self.q, self.zp = self.z // PAIR, self.z % PAIR
        self.x, self.c = tp // CORES, tp % CORES
        self.chips = PAIR * self.nx

    def z_at(self, i):
        q = (self.q + i // PAIR) % self.nq
        return q * PAIR + (self.zp + i % PAIR) % PAIR

    def f_at(self, i, j):
        return self.z_at(i) * self.ny + (self.y + j) % self.ny

    def at_z(self, z):
        return (z * self.ny + self.y, self.tp)

    def at_y(self, j):
        return (self.z * self.ny + (self.y + j) % self.ny, self.tp)

    def at_x(self, s):
        return (self.fs, ((self.x + s) % self.nx) * CORES + self.c)

    def other_z(self):
        return self.at_z(self.q * PAIR + 1 - self.zp)

    def other_core(self):
        return (self.fs, self.x * CORES + 1 - self.c)


def remote(src, dst, send, recv, device):
    return pltpu.make_async_remote_copy(
        src_ref=src, dst_ref=dst, send_sem=send, recv_sem=recv, device_id=device, device_id_type=MESH
    )


def layer_kernel(n, t, *refs):
    (tokens, gain1, gainm, gain2, taps, gate_a, gate_x, slope) = refs[:8]
    sources = (refs[8:11], refs[11:14], refs[14:17])
    out = refs[17]
    (w1, wm, w2, rows_of, xs, xr, ys, yr, zs, zr, own, part, hid, acc, hid_m, acc_m, res) = refs[18:35]
    (rw, zsend, ysend, lsem, gr, gs, xss, xsr, yss, ysr, zss, zsr) = refs[35:]
    weights = (w1, wm, w2)
    me = Place(n, t)
    r, dn = tokens.shape[1], tokens.shape[2]
    width = n * dn
    chips, nx, ny, nz = me.chips, me.nx, me.ny, me.nz
    mine = me.zp * nx + me.x
    rest = (1 - me.zp) * nx + me.x

    barrier = pltpu.get_barrier_semaphore()
    peers = [me.at_z((me.z + d) % nz) for d in range(1, nz)]
    peers += [me.at_y(j) for j in range(1, ny)]
    peers += [me.at_x(s) for s in range(1, nx)]
    peers += [me.other_core()]
    for peer in peers:
        pl.semaphore_signal(barrier, inc=1, device_id=peer, device_id_type=MESH)
    pl.semaphore_wait(barrier, len(peers))

    def z_piece(s, k, i):
        z = me.z_at(i)
        return remote(
            sources[s][k].at[z % PAIR],
            weights[s].at[k, me.fs],
            zsend.at[s, k, i],
            rw.at[s, k, me.fs],
            me.at_z(z),
        )

    def y_piece(s, k, i, j):
        f = me.f_at(i, 0)
        src = sources[s][k].at[me.zp] if isinstance(i, int) and i == 0 else weights[s].at[k, f]
        return remote(
            src, weights[s].at[k, f], ysend.at[s, k, i, j], rw.at[s, k, f], me.at_y(j)
        )

    def local_piece(s, k):
        return pltpu.make_async_copy(
            sources[s][k].at[me.zp], weights[s].at[k, me.fs], lsem.at[s, k]
        )

    def arrived(s, k, f):
        place = weights[s].at[k, f]
        remote(place, place, zsend.at[s, k, 0], rw.at[s, k, f], me.at_y(0)).wait_recv()

    def send_weights(s, k):
        for i in list(range(PAIR, nz)) + [1]:
            z_piece(s, k, i).start()
        for j in range(1, ny):
            y_piece(s, k, 0, j).start()
        local_piece(s, k).start()

    def forward(s, k, i):
        arrived(s, k, me.f_at(i, 0))
        for j in range(1, ny):
            y_piece(s, k, i, j).start()

    def collect(s, k):
        for i in range(nz):
            for j in range(1, ny):
                arrived(s, k, me.f_at(i, j))
        local_piece(s, k).wait()

    def row_block(g, p, c):
        return rows_of.at[g, p, c]

    def row_copy(g, p, c, slot, device):
        block = row_block(g, p, c)
        return remote(block, block, gs.at[g, slot], gr.at[g, p, c], device)

    def row_wait(g, p, c):
        block = row_block(g, p, c)
        remote(block, block, gs.at[g, 0], gr.at[g, p, c], me.other_core()).wait_recv()

    def norm_rows(values, gain):
        total = jnp.zeros((r, 1), jnp.float32)
        for f in range(n):
            wide = values(f)
            total += jnp.sum(wide * wide, axis=-1, keepdims=True)
        scale = lax.rsqrt(total / width + EPS)
        return lambda f: (values(f) * scale * gain[f]).astype(jnp.bfloat16)

    row_sends = []

    def send_rows(g, values, gain):
        normed = norm_rows(values, gain)
        for f in range(n):
            rows_of[g, mine, me.c, f] = normed(f)
        copies = [row_copy(g, mine, me.c, 0, me.other_z())]
        copies += [row_copy(g, mine, me.c, s, me.at_x(s)) for s in range(1, nx)]
        copies += [row_copy(g, mine, me.c, nx, me.other_core())]
        for copy in copies:
            copy.start()
        row_sends.extend(copies)

    def get_rows(g):
        slot = nx + 1
        moves = [(rest, True)]
        moves += [(me.zp * nx + (me.x + s) % nx, False) for s in range(1, nx)]
        moves += [((1 - me.zp) * nx + (me.x + s) % nx, False) for s in range(1, nx)]
        for p, across in moves:
            row_wait(g, p, me.c)
            copies = []
            if across:
                for s in range(1, nx):
                    copies.append(row_copy(g, p, me.c, slot, me.at_x(s)))
                    slot += 1
            copies.append(row_copy(g, p, me.c, slot, me.other_core()))
            slot += 1
            for copy in copies:
                copy.start()
            row_sends.extend(copies)
        for p in range(chips):
            row_wait(g, p, 1 - me.c)

    def core_part(g, f):
        return remote(xs.at[f], xr.at[f], xss.at[g, f], xsr.at[g, f], me.other_core())

    def x_part(g, f, s):
        return remote(
            ys.at[f, s - 1], yr.at[f, s - 1], yss.at[g, f, s - 1], ysr.at[g, f, s - 1], me.at_x(s)
        )

    def z_part(g, f):
        return remote(zs.at[f], zr.at[f], zss.at[g, f], zsr.at[g, f], me.other_z())

    def reduce_rows(g, s, hidden):
        last = MATS - 1

        def use(f):
            weight = weights[s][last, f]
            term = jnp.dot(hidden[1 - me.c], weight, preferred_element_type=jnp.float32)
            xs[f] = term.astype(jnp.bfloat16).reshape(chips, r, dn)
            core_part(g, f).start()
            term = jnp.dot(hidden[me.c], weight, preferred_element_type=jnp.float32)
            core_part(g, f).wait_recv()
            part[...] = term.reshape(chips, r, dn) + xr[f].astype(jnp.float32)
            for d in range(1, nx):
                for h in range(PAIR):
                    ys[f, d - 1, h] = part[h * nx + (me.x + d) % nx].astype(jnp.bfloat16)
                x_part(g, f, d).start()
            for h in range(PAIR):
                own[f, h] = part[h * nx + me.x]

        def pass_on(f):
            total = own[f, 1 - me.zp]
            for d in range(1, nx):
                x_part(g, f, d).wait_recv()
                total = total + yr[f, d - 1, 1 - me.zp].astype(jnp.float32)
            zs[f] = total.astype(jnp.bfloat16)
            z_part(g, f).start()

        def step(i, carry):
            @pl.when(i < nz)
            def _():
                @pl.when(i > 0)
                def _():
                    f = me.f_at(i, 0)
                    arrived(s, last, f)
                    for j in range(1, ny):
                        remote(
                            weights[s].at[last, f],
                            weights[s].at[last, f],
                            ysend.at[s, last, i, j],
                            rw.at[s, last, f],
                            me.at_y(j),
                        ).start()

                @pl.when(i == 0)
                def _():
                    local_piece(s, last).wait()

                use(me.f_at(i, 0))

            @pl.when((i >= 1) & (i <= nz))
            def _():
                for j in range(1, ny):
                    f = me.f_at(i - 1, j)
                    arrived(s, last, f)
                    use(f)
                pass_on(me.f_at(i - 1, 0))

            @pl.when(i >= 2)
            def _():
                for j in range(1, ny):
                    pass_on(me.f_at(i - 2, j))

            return carry

        lax.fori_loop(0, nz + 2, step, 0)

    def drain(g):
        def one(f, carry):
            core_part(g, f).wait_send()
            for d in range(1, nx):
                x_part(g, f, d).wait_send()
            z_part(g, f).wait_send()
            return carry

        lax.fori_loop(0, n, one, 0)

    def reduced(g, f):
        z_part(g, f).wait_recv()
        total = own[f, me.zp]
        for d in range(1, nx):
            total = total + yr[f, d - 1, me.zp].astype(jnp.float32)
        return total + zr[f].astype(jnp.float32)

    def hidden_rows(g, s):
        def side(c, carry):
            acc[...] = jnp.zeros_like(acc)

            def feature(f, carry):
                rows = rows_of[g, :, c, f].reshape(chips * r, dn)
                for k in range(MATS - 1):
                    acc[k] += dot_nt(rows, weights[s][k, f])
                return carry

            lax.fori_loop(0, n, feature, 0)
            gate = acc[0]
            hid[c] = (gate * sigmoid(gate) * acc[1]).astype(jnp.bfloat16)
            return carry

        lax.fori_loop(0, CORES, side, 0)

    def mix_rows(g, s):
        acc_m[...] = jnp.zeros_like(acc_m)
        length = nx * CORES * r

        def feature(f, carry):
            rows = rows_of[g, :, :, f].reshape(PAIR * length, dn)
            for k in range(MATS - 1):
                acc_m[k] += dot_nt(rows, weights[s][k, f])
            return carry

        lax.fori_loop(0, n, feature, 0)
        tap = taps[me.zp].astype(jnp.float32)
        a, b = gate_a[me.zp], gate_x[me.zp]
        fall = slope[me.zp]
        for q in range(PAIR):
            rows = pl.ds(q * length, length)
            lru = acc_m[0, rows].astype(jnp.bfloat16).astype(jnp.float32)
            gated = acc_m[1, rows].astype(jnp.bfloat16).astype(jnp.float32)
            conv = tap[0:1] * lru
            for k in range(1, tap.shape[0]):
                conv = conv + tap[k : k + 1] * shift_down(lru, k, 0.0)
            low = conv.astype(jnp.bfloat16)
            recall = sigmoid(jnp.dot(low, a, preferred_element_type=jnp.float32))
            admit = sigmoid(jnp.dot(low, b, preferred_element_type=jnp.float32))
            log_keep = -8.0 * recall * fall
            keep = jnp.exp(log_keep)
            grow = -jnp.tanh(log_keep) * (1.0 + keep * keep)
            state = jnp.sqrt(grow) * admit * low.astype(jnp.float32)
            step = 1
            while step < length:
                state = state + keep * shift_down(state, step, 0.0)
                keep = keep * shift_down(keep, step, 1.0)
                step *= 2
            inner = 0.7978845608028654 * (gated + 0.044715 * gated * gated * gated)
            mixed = state * (0.5 * gated * (1.0 + jnp.tanh(inner)))
            mixed = mixed.astype(jnp.bfloat16)
            for x in range(nx):
                for c in range(CORES):
                    at = (x * CORES + c) * r
                    hid_m[c, pl.ds((q * nx + x) * r, r)] = mixed[at : at + r]

    send_rows(0, lambda f: tokens[f].astype(jnp.float32), gain1)
    for s in range(2):
        for k in range(MATS):
            send_weights(s, k)
    get_rows(0)
    for k in range(MATS - 1):
        for i in range(1, nz):
            forward(0, k, i)
    for k in range(MATS - 1):
        collect(0, k)
    hidden_rows(0, 0)
    reduce_rows(0, 0, hid)
    send_weights(2, 0)
    for f in range(n):
        res[f] = (tokens[f].astype(jnp.float32) + 0.5 * reduced(0, f)).astype(jnp.bfloat16)
    send_rows(1, lambda f: res[f].astype(jnp.float32), gainm)
    send_weights(2, 1)
    for k in range(MATS - 1):
        for i in range(1, nz):
            forward(1, k, i)
    get_rows(1)
    for k in range(MATS - 1):
        collect(1, k)
    mix_rows(1, 1)
    drain(0)
    reduce_rows(1, 1, hid_m)
    send_weights(2, 2)
    for i in range(1, nz):
        forward(2, 0, i)
    for f in range(n):
        res[f] = (res[f].astype(jnp.float32) + reduced(1, f)).astype(jnp.bfloat16)
    send_rows(2, lambda f: res[f].astype(jnp.float32), gain2)
    get_rows(2)
    for i in range(1, nz):
        forward(2, 1, i)
    for k in range(MATS - 1):
        collect(2, k)
    hidden_rows(2, 2)
    drain(1)
    reduce_rows(2, 2, hid)
    for f in range(n):
        out[f] = (res[f].astype(jnp.float32) + 0.5 * reduced(2, f)).astype(jnp.bfloat16)

    for copy in row_sends:
        copy.wait_send()
    for s in range(3):
        for k in range(MATS):
            for i in range(1, nz):
                z_piece(s, k, i).wait_send()
            for i in range(nz):
                for j in range(1, ny):
                    y_piece(s, k, i, j).wait_send()

    drain(2)


def body(
    n,
    t,
    tokens,
    ffn1_gain,
    ffn1_gate,
    ffn1_up,
    ffn1_down,
    mix_gain,
    lru_in_weight,
    lru_gate_weight,
    conv_weight,
    gate_a_weight,
    gate_x_weight,
    decay_param,
    mix_out_weight,
    ffn2_gain,
    ffn2_gate,
    ffn2_up,
    ffn2_down,
):
    r, width = tokens.shape
    dn = width // n
    ny = math.isqrt(n // PAIR)
    nz, nx = n // ny, t // CORES
    chips = PAIR * nx
    hs = ffn1_gate.shape[1] // PAIR
    size = gate_a_weight.shape[1]
    extra = -gate_a_weight.shape[0] % PAIR
    if extra:
        lru_in_weight, lru_gate_weight, conv_weight = (
            jnp.pad(w, ((0, 0), (0, extra * size))) for w in (lru_in_weight, lru_gate_weight, conv_weight)
        )
        gate_a_weight, gate_x_weight = (
            jnp.pad(w, ((0, extra), (0, 0), (0, 0))) for w in (gate_a_weight, gate_x_weight)
        )
        decay_param = jnp.pad(decay_param, (0, extra * size))
        mix_out_weight = jnp.pad(mix_out_weight, ((0, extra * size), (0, 0)))
    cs = lru_in_weight.shape[1] // PAIR
    count = gate_a_weight.shape[0] // PAIR

    def halves(first, second, third):
        return [w.reshape(PAIR, -1, dn) for w in (first.T, second.T, third)]

    def blocks(v):
        return v.reshape(n, 1, dn)

    eye = jnp.eye(count, dtype=jnp.bfloat16)

    def dense(weight):
        weight = weight.reshape(PAIR, count, size, size)
        return (eye[:, None, :, None] * weight[:, :, :, None, :]).reshape(PAIR, cs, cs)

    small = [
        tokens.reshape(r, n, dn).transpose(1, 0, 2),
        blocks(ffn1_gain),
        blocks(mix_gain),
        blocks(ffn2_gain),
        conv_weight.reshape(-1, PAIR, cs).transpose(1, 0, 2),
        dense(gate_a_weight),
        dense(gate_x_weight),
        jax.nn.softplus(-decay_param).reshape(PAIR, 1, cs),
    ]
    big = (
        halves(ffn1_gate, ffn1_up, ffn1_down)
        + halves(lru_in_weight, lru_gate_weight, mix_out_weight)
        + halves(ffn2_gate, ffn2_up, ffn2_down)
    )
    bf16, f32 = jnp.bfloat16, jnp.float32
    sem = pltpu.SemaphoreType.DMA
    scratch = [
        pltpu.VMEM((MATS, n, hs, dn), bf16),
        pltpu.VMEM((MATS, n, cs, dn), bf16),
        pltpu.VMEM((MATS, n, hs, dn), bf16),
        pltpu.VMEM((3, chips, CORES, n, r, dn), bf16),
        pltpu.VMEM((n, chips, r, dn), bf16),
        pltpu.VMEM((n, chips, r, dn), bf16),
        pltpu.VMEM((n, nx - 1, PAIR, r, dn), bf16),
        pltpu.VMEM((n, nx - 1, PAIR, r, dn), bf16),
        pltpu.VMEM((n, r, dn), bf16),
        pltpu.VMEM((n, r, dn), bf16),
        pltpu.VMEM((n, PAIR, r, dn), f32),
        pltpu.VMEM((chips, r, dn), f32),
        pltpu.VMEM((CORES, chips * r, hs), bf16),
        pltpu.VMEM((MATS - 1, chips * r, hs), f32),
        pltpu.VMEM((CORES, chips * r, cs), bf16),
        pltpu.VMEM((MATS - 1, CORES * chips * r, cs), f32),
        pltpu.VMEM((n, r, dn), bf16),
        sem((3, MATS, n)),
        sem((3, MATS, nz)),
        sem((3, MATS, nz, ny)),
        sem((3, MATS)),
        sem((3, chips, CORES)),
        sem((3, 4 * nx)),
        sem((3, n)),
        sem((3, n)),
        sem((3, n, nx - 1)),
        sem((3, n, nx - 1)),
        sem((3, n)),
        sem((3, n)),
    ]
    vmem = pl.BlockSpec(memory_space=pltpu.VMEM)
    hbm = pl.BlockSpec(memory_space=pl.ANY)
    result = pl.pallas_call(
        functools.partial(layer_kernel, n, t),
        out_shape=jax.ShapeDtypeStruct((n, r, dn), bf16),
        in_specs=[vmem] * len(small) + [hbm] * len(big),
        out_specs=vmem,
        scratch_shapes=scratch,
        compiler_params=pltpu.CompilerParams(
            collective_id=0, has_side_effects=True, vmem_limit_bytes=66_000_000
        ),
    )(*small, *big)
    return result.transpose(1, 0, 2).reshape(r, width)


def solution(mesh):
    n, t = mesh.shape["fs"], mesh.shape["tp"]
    in_specs = (
        P(("fs", "tp"), None),
        P(),
        P("fs", "tp"),
        P("fs", "tp"),
        P("tp", "fs"),
        P(),
        P("fs", "tp"),
        P("fs", "tp"),
        P(None, "tp"),
        P("tp", None, None),
        P("tp", None, None),
        P("tp"),
        P("tp", "fs"),
        P(),
        P("fs", "tp"),
        P("fs", "tp"),
        P("tp", "fs"),
    )

    def run(*args):
        return body(n, t, *args)

    return jax.shard_map(
        run, mesh=mesh, in_specs=in_specs, out_specs=P(("fs", "tp"), None), check_vma=False
    )
```

```python
import functools
import math

import jax
import jax.numpy as jnp
from jax import lax
from jax.experimental import pallas as pl
from jax.experimental.pallas import tpu as pltpu
from jax.sharding import PartitionSpec as P

EPS = 1e-06
CORES = 2
PAIR = 2
MATS = 3
ROW_PARTS = 4
MESH = pl.DeviceIdType.MESH


def dot_nt(a, b):
    return lax.dot_general(a, b, (((1,), (1,)), ((), ())), preferred_element_type=jnp.float32)


def sigmoid(v):
    return 1.0 / (1.0 + jnp.exp(-v))


def shift_down(values, step, fill):
    pad = jnp.full((step, values.shape[1]), fill, values.dtype)
    return jnp.concatenate([pad, values[: values.shape[0] - step]], axis=0)


class Place:
    def __init__(self, n, t):
        self.n, self.t = n, t
        self.ny = math.isqrt(n // PAIR)
        self.nz = n // self.ny
        self.nq = self.nz // PAIR
        self.nx = t // CORES
        fs, tp = lax.axis_index("fs"), lax.axis_index("tp")
        self.fs, self.tp = fs, tp
        self.z, self.y = fs // self.ny, fs % self.ny
        self.q, self.zp = self.z // PAIR, self.z % PAIR
        self.x, self.c = tp // CORES, tp % CORES
        self.chips = PAIR * self.nx
        self.inner = (self.q + self.zp) % PAIR

    def z_at(self, i):
        q = (self.q + i // PAIR) % self.nq
        turn = self.inner * (1 if i >= PAIR else 0) if isinstance(i, int) else jnp.where(i >= PAIR, self.inner, 0)
        return q * PAIR + (self.zp + i + turn) % PAIR

    def f_at(self, i, j):
        return self.z_at(i) * self.ny + (self.y + j) % self.ny

    def at_z(self, z):
        return (z * self.ny + self.y, self.tp)

    def at_y(self, j):
        return (self.z * self.ny + (self.y + j) % self.ny, self.tp)

    def at_x(self, s):
        return (self.fs, ((self.x + s) % self.nx) * CORES + self.c)

    def other_z(self):
        return self.at_z(self.q * PAIR + 1 - self.zp)

    def other_core(self):
        return (self.fs, self.x * CORES + 1 - self.c)


def remote(src, dst, send, recv, device):
    return pltpu.make_async_remote_copy(
        src_ref=src, dst_ref=dst, send_sem=send, recv_sem=recv, device_id=device, device_id_type=MESH
    )


def layer_kernel(n, t, *refs):
    (tokens_in, gain1, gainm, gain2, taps, gate_a, gate_x, slope) = refs[:8]
    raw = (refs[8:11], refs[11:14], refs[14:17])
    out = refs[17]
    (w1, wm, w2, rel1, relm, rel2, rows_of, xs, xr, ys, yr, zs, zr, own, part_sum, hid, acc, hid_m, acc_m, res, tokens, load1, loadm, load2, flip1, flipm, flip2, wide_a, wide_x) = refs[18:47]
    (rw, rrel, zsend, ysend, lsem, gr, gs, xss, xsr, yss, ysr, zss, zsr, load_sem) = refs[47:]
    weights = (w1, wm, w2)
    relays = (rel1, relm, rel2)
    me = Place(n, t)
    r, width = tokens_in.shape
    dn = width // n
    loads, flips = (load1, loadm, load2), (flip1, flipm, flip2)
    sources = [
        [flips[s].at[k] for k in range(MATS - 1)]
        + [raw[s][MATS - 1]]
        for s in range(3)
    ]

    def load(s, k):
        return pltpu.make_async_copy(raw[s][k], loads[s].at[k], load_sem.at[s, k])

    def flip(s, k):
        load(s, k).wait()
        flips[s][k] = loads[s][k].T.reshape(flips[s].shape[1:])

    for s in range(3):
        for k in range(MATS - 1):
            load(s, k).start()
    chips, nx, ny, nz = me.chips, me.nx, me.ny, me.nz
    parts = math.gcd(n, ROW_PARTS)
    step = n // parts
    mine = me.zp * nx + me.x
    rest = (1 - me.zp) * nx + me.x

    barrier = pltpu.get_barrier_semaphore()
    peers = [me.at_z((me.z + d) % nz) for d in range(1, nz)]
    peers += [me.at_y(j) for j in range(1, ny)]
    peers += [me.at_x(s) for s in range(1, nx)]
    peers += [me.other_core()]
    for peer in peers:
        pl.semaphore_signal(barrier, inc=1, device_id=peer, device_id_type=MESH)
    flip(0, 0)
    for f in range(n):
        tokens[f] = tokens_in[:, f * dn : (f + 1) * dn]
    pl.semaphore_wait(barrier, len(peers))

    def z_piece(s, k, i):
        z = me.z_at(i)
        return remote(
            sources[s][k].at[z % PAIR],
            weights[s].at[k, me.fs],
            zsend.at[s, k, i],
            rw.at[s, k, me.fs],
            me.at_z(z),
        )

    def y_piece(s, k, i, j):
        f = me.f_at(i, 0)
        src = sources[s][k].at[me.zp] if isinstance(i, int) and i == 0 else weights[s].at[k, f]
        return remote(
            src, weights[s].at[k, f], ysend.at[s, k, i, j], rw.at[s, k, f], me.at_y(j)
        )

    def local_piece(s, k):
        return pltpu.make_async_copy(
            sources[s][k].at[me.zp], weights[s].at[k, me.fs], lsem.at[s, k]
        )

    def arrived(s, k, f):
        place = weights[s].at[k, f]
        remote(place, place, zsend.at[s, k, 0], rw.at[s, k, f], me.at_y(0)).wait_recv()

    def relay_in(s, k):
        return remote(
            sources[s][k].at[me.zp],
            relays[s].at[k],
            zsend.at[s, k, 0],
            rrel.at[s, k],
            me.other_z(),
        )

    def relay_near(s, k, i):
        f = me.f_at(1, 0)
        place = weights[s].at[k, f]
        return remote(place, place, zsend.at[s, k, nz + i], rw.at[s, k, f], me.at_z(me.z_at(i)))

    def relay_out(s, k, i):
        f = me.f_at(1, 0)
        return remote(
            relays[s].at[k],
            weights[s].at[k, f],
            zsend.at[s, k, nz + i],
            rw.at[s, k, f],
            me.at_z(me.z_at(i)),
        )

    def when_inner(*actions):
        @pl.when(me.inner == 1)
        def _():
            for act, s, k in actions:
                act(s, k)

    def when_end(*actions):
        @pl.when(me.inner == 0)
        def _():
            for act, s, k in actions:
                act(s, k)

    def send_cross(s, k):
        for i in range(PAIR, nz):
            z_piece(s, k, i).start()

    def send_near(s, k):
        z_piece(s, k, 1).start()

    def send_both(s, k):
        send_near(s, k)
        relay_in(s, k).start()

    def relay(s, k):
        relay_in(s, k).wait_recv()
        for i in range(PAIR, nz, 2):
            relay_out(s, k, i).start()

    def send_own(s, k):
        for j in range(1, ny):
            y_piece(s, k, 0, j).start()
        local_piece(s, k).start()

    def forward(s, k, i):
        arrived(s, k, me.f_at(i, 0))
        for j in range(1, ny):
            y_piece(s, k, i, j).start()
        if i == 1:

            @pl.when(me.inner == 1)
            def _():
                for m in range(PAIR + 1, nz, 2):
                    relay_near(s, k, m).start()

    def collect(s, k):
        local_piece(s, k).wait()
        for i in range(nz):
            for j in range(1, ny):
                arrived(s, k, me.f_at(i, j))

    def row_copy(g, p, c, slot, part, device):
        block = rows_of.at[g, p, c, pl.ds(part * step, step)]
        return remote(block, block, gs.at[g, slot, part], gr.at[g, p, c, part], device)

    def row_wait(g, p, c, part):
        row_copy(g, p, c, 0, part, me.other_core()).wait_recv()

    def norm_rows(values, gain):
        total = jnp.zeros((r, 1), jnp.float32)
        for f in range(n):
            wide = values(f)
            total += jnp.sum(wide * wide, axis=-1, keepdims=True)
        scale = lax.rsqrt(total / width + EPS)
        return lambda f: (values(f) * scale * gain[:, f * dn : (f + 1) * dn]).astype(jnp.bfloat16)

    row_sends = []

    def send_rows(g, values, gain):
        normed = norm_rows(values, gain)
        for f in range(n):
            rows_of[g, mine, me.c, f] = normed(f)
        targets = [me.other_z()] + [me.at_x(d) for d in range(1, nx)] + [me.other_core()]
        for slot, device in enumerate(targets):
            for part in range(parts):
                copy = row_copy(g, mine, me.c, slot, part, device)
                copy.start()
                row_sends.append(copy)

    def spread(g, p, slot, part, across):
        row_wait(g, p, me.c, part)
        targets = [me.at_x(d) for d in range(1, nx)] if across else []
        targets += [me.other_core()]
        for m, device in enumerate(targets):
            copy = row_copy(g, p, me.c, slot + m, part, device)
            copy.start()
            row_sends.append(copy)

    def near_rows(g):
        for part in range(parts):
            spread(g, rest, nx + 1, part, True)

    def far_rows(g):
        slot = 2 * nx + 1
        for base in (me.zp * nx, (1 - me.zp) * nx):
            for d in range(1, nx):
                for part in range(parts):
                    spread(g, base + (me.x + d) % nx, slot, part, False)
                slot += 1
        for p in range(chips):
            for part in range(parts):
                row_wait(g, p, 1 - me.c, part)

    def core_part(g, f):
        return remote(xs.at[f], xr.at[f], xss.at[g, f], xsr.at[g, f], me.other_core())

    def x_part(g, f, s):
        return remote(
            ys.at[f, s - 1], yr.at[f, s - 1], yss.at[g, f, s - 1], ysr.at[g, f, s - 1], me.at_x(s)
        )

    def z_part(g, f):
        return remote(zs.at[f], zr.at[f], zss.at[g, f], zsr.at[g, f], me.other_z())

    order = [(0, 0)]
    for i in range(1, nz + 1):
        order += [(i, 0)] if i < nz else []
        order += [(i - 1, j) for j in range(1, ny)]

    def reduce_rows(g, s, hidden, early=(), paced=False):
        last = MATS - 1

        def begin(m):
            i, j = order[m]
            f = me.f_at(i, j)
            if j:
                arrived(s, last, f)
            elif i == 0:
                local_piece(s, last).wait()
            elif i not in early:
                forward(s, last, i)
            weight = weights[s][last, f]
            term = jnp.dot(hidden[1 - me.c], weight, preferred_element_type=jnp.float32)
            xs[f] = term.astype(jnp.bfloat16).reshape(chips, r, dn)
            core_part(g, f).start()
            term = jnp.dot(hidden[me.c], weight, preferred_element_type=jnp.float32)
            part_sum[m % 2] = term.reshape(chips, r, dn)

        def cross(m):
            f = me.f_at(*order[m])
            core_part(g, f).wait_recv()
            for h in range(PAIR):
                for d in range(1, nx):
                    p = h * nx + (me.x + d) % nx
                    total = part_sum[m % 2, p] + xr[f, p].astype(jnp.float32)
                    ys[f, d - 1, h] = total.astype(jnp.bfloat16)
            for d in range(1, nx):
                x_part(g, f, d).start()
            for h in range(PAIR):
                p = h * nx + me.x
                own[f, h] = part_sum[m % 2, p] + xr[f, p].astype(jnp.float32)

        def pass_on(m):
            f = me.f_at(*order[m])
            total = own[f, 1 - me.zp]
            for d in range(1, nx):
                x_part(g, f, d).wait_recv()
                total = total + yr[f, d - 1, 1 - me.zp].astype(jnp.float32)
            zs[f] = total.astype(jnp.bfloat16)
            z_part(g, f).start()

        for m in range(n + 3):
            if paced and 1 <= m <= n:
                cross(m - 1)
            if m < n:
                begin(m)
            if not paced and 1 <= m <= n:
                cross(m - 1)
            if m >= 3:
                pass_on(m - 3)

    def reduced(g, f):
        z_part(g, f).wait_recv()
        total = own[f, me.zp]
        for d in range(1, nx):
            total = total + yr[f, d - 1, me.zp].astype(jnp.float32)
        return total + zr[f].astype(jnp.float32)

    def drain(g):
        def one(f, carry):
            core_part(g, f).wait_send()
            for d in range(1, nx):
                x_part(g, f, d).wait_send()
            z_part(g, f).wait_send()
            return carry

        lax.fori_loop(0, n, one, 0)

    def project(g, s, k, c, to):
        acc[to] = jnp.zeros_like(acc[to])

        def feature(f, carry):
            rows = rows_of[g, :, c, f].reshape(chips * r, dn)
            acc[to] += dot_nt(rows, weights[s][k, f])
            return carry

        lax.fori_loop(0, n, feature, 0)

    def gate_rows(g, s):
        def side(c, carry):
            project(g, s, 0, c, c)
            return carry

        lax.fori_loop(0, CORES, side, 0)

    def hidden_rows(g, s):
        def side(c, carry):
            project(g, s, 1, c, CORES)
            gate = acc[c]
            hid[c] = (gate * sigmoid(gate) * acc[CORES]).astype(jnp.bfloat16)
            return carry

        lax.fori_loop(0, CORES, side, 0)

    def mix_rows(g, s):
        acc_m[...] = jnp.zeros_like(acc_m)
        length = nx * CORES * r

        def feature(f, carry):
            rows = rows_of[g, :, :, f].reshape(PAIR * length, dn)
            for k in range(MATS - 1):
                acc_m[k] += dot_nt(rows, weights[s][k, f])
            return carry

        lax.fori_loop(0, n, feature, 0)
        channels = taps.shape[1] // PAIR

        def mine_of(v):
            return jnp.where(me.zp == 0, v[:, :channels], v[:, channels:])

        tap = mine_of(taps[...].astype(jnp.float32))
        fall = mine_of(slope[...])
        count, size = gate_a.shape[0] // PAIR, gate_a.shape[1]
        for wide, gate in ((wide_a, gate_a), (wide_x, gate_x)):
            wide[...] = jnp.zeros_like(wide)
            for m in range(count):
                at = slice(m * size, (m + 1) * size)
                wide[at, at] = gate[me.zp * count + m].astype(jnp.float32)
        a, b = wide_a[...].astype(jnp.bfloat16), wide_x[...].astype(jnp.bfloat16)
        for q in range(PAIR):
            rows = pl.ds(q * length, length)
            lru = acc_m[0, rows].astype(jnp.bfloat16).astype(jnp.float32)
            gated = acc_m[1, rows].astype(jnp.bfloat16).astype(jnp.float32)
            conv = tap[0:1] * lru
            for k in range(1, tap.shape[0]):
                conv = conv + tap[k : k + 1] * shift_down(lru, k, 0.0)
            low = conv.astype(jnp.bfloat16)
            recall = sigmoid(jnp.dot(low, a, preferred_element_type=jnp.float32))
            admit = sigmoid(jnp.dot(low, b, preferred_element_type=jnp.float32))
            log_keep = -8.0 * recall * fall
            keep = jnp.exp(log_keep)
            grow = -jnp.tanh(log_keep) * (1.0 + keep * keep)
            state = jnp.sqrt(grow) * admit * low.astype(jnp.float32)
            step = 1
            while step < length:
                state = state + keep * shift_down(state, step, 0.0)
                keep = keep * shift_down(keep, step, 1.0)
                step *= 2
            inner = 0.7978845608028654 * (gated + 0.044715 * gated * gated * gated)
            mixed = state * (0.5 * gated * (1.0 + jnp.tanh(inner)))
            mixed = mixed.astype(jnp.bfloat16)
            for x in range(nx):
                for c in range(CORES):
                    at = (x * CORES + c) * r
                    hid_m[c, pl.ds((q * nx + x) * r, r)] = mixed[at : at + r]

    first = range(PAIR, nz, PAIR)
    second = range(PAIR + 1, nz, PAIR)

    def forward_all(s, k, which):
        for i in which:
            forward(s, k, i)

    when_end((send_both, 0, 0))
    when_inner((send_near, 0, 0), (send_cross, 0, 0))
    send_own(0, 0)
    send_rows(0, lambda f: tokens[f].astype(jnp.float32), gain1)
    flip(0, 1)
    when_end((send_both, 0, 1), (send_both, 0, 2))
    when_inner((send_near, 0, 1), (send_near, 0, 2), (send_cross, 0, 1))
    send_own(0, 1)
    send_own(0, 2)
    for s in (1, 2):
        for k in range(MATS - 1):
            flip(s, k)
    for k in range(MATS):
        send_own(1, k)
    send_own(2, 0)
    forward_all(0, 0, [1])
    when_inner((relay, 0, 0), (send_cross, 0, 2))
    near_rows(0)
    forward_all(0, 0, first)
    far_rows(0)
    forward_all(0, 0, second)
    forward_all(0, 1, [1])
    when_inner((relay, 0, 1), (send_near, 2, 0))
    collect(0, 0)
    when_end(*[(send_both, 1, k) for k in range(MATS)], (send_both, 2, 0), (send_both, 2, 1))
    gate_rows(0, 0)
    forward_all(0, 1, first)
    forward_all(0, 2, [1])
    when_inner((relay, 0, 2))
    forward_all(0, 1, second)
    when_inner(*[(act, 1, k) for k in range(MATS) for act in (send_near, send_cross, relay)])
    collect(0, 1)
    for k in range(MATS):
        forward_all(1, k, [1])
    when_inner((send_near, 2, 1))
    hidden_rows(0, 0)
    reduce_rows(0, 0, hid, [1], True)
    when_inner((send_cross, 2, 0), (send_cross, 2, 1), (send_cross, 2, 2))
    for f in range(n):
        res[f] = (tokens[f].astype(jnp.float32) + 0.5 * reduced(0, f)).astype(jnp.bfloat16)
    send_rows(1, lambda f: res[f].astype(jnp.float32), gainm)
    when_end((send_both, 2, 2))
    for k in range(MATS):
        forward_all(1, k, range(2, nz))
    forward_all(2, 0, [1])
    when_inner((relay, 2, 0), (relay, 2, 1))
    near_rows(1)
    when_inner((send_near, 2, 2))
    send_own(2, 1)
    far_rows(1)
    for k in range(MATS - 1):
        collect(1, k)
    forward_all(2, 1, [1])
    mix_rows(1, 1)
    forward_all(2, 0, first)
    send_own(2, 2)
    drain(0)
    reduce_rows(1, 1, hid_m, range(1, nz))
    forward_all(2, 2, [1])
    when_inner((relay, 2, 2))
    forward_all(2, 1, first)
    for f in range(n):
        res[f] = (res[f].astype(jnp.float32) + reduced(1, f)).astype(jnp.bfloat16)
    send_rows(2, lambda f: res[f].astype(jnp.float32), gain2)
    forward_all(2, 2, first)
    forward_all(2, 0, second)
    near_rows(2)
    far_rows(2)
    forward_all(2, 1, second)
    collect(2, 0)
    gate_rows(2, 2)
    collect(2, 1)
    hidden_rows(2, 2)
    drain(1)
    reduce_rows(2, 2, hid, [1, *first], True)
    for f in range(n):
        out[f] = (res[f].astype(jnp.float32) + 0.5 * reduced(2, f)).astype(jnp.bfloat16)

    for copy in row_sends:
        copy.wait_send()
    for s in range(3):
        for k in range(MATS):
            z_piece(s, k, 1).wait_send()
            for i in range(nz):
                for j in range(1, ny):
                    y_piece(s, k, i, j).wait_send()

    def finish_inner(s, k):
        for i in range(PAIR, nz):
            z_piece(s, k, i).wait_send()
            (relay_near if i % PAIR else relay_out)(s, k, i).wait_send()

    def finish_end(s, k):
        relay_in(s, k).wait_send()

    when_inner(*[(finish_inner, s, k) for s in range(3) for k in range(MATS)])
    when_end(*[(finish_end, s, k) for s in range(3) for k in range(MATS)])

    drain(2)


def body(
    n,
    t,
    tokens,
    ffn1_gain,
    ffn1_gate,
    ffn1_up,
    ffn1_down,
    mix_gain,
    lru_in_weight,
    lru_gate_weight,
    conv_weight,
    gate_a_weight,
    gate_x_weight,
    decay_param,
    mix_out_weight,
    ffn2_gain,
    ffn2_gate,
    ffn2_up,
    ffn2_down,
):
    r, width = tokens.shape
    dn = width // n
    ny = math.isqrt(n // PAIR)
    nz, nx = n // ny, t // CORES
    chips = PAIR * nx
    parts = math.gcd(n, ROW_PARTS)
    hs = ffn1_gate.shape[1] // PAIR
    size = gate_a_weight.shape[1]
    extra = -gate_a_weight.shape[0] % PAIR
    if extra:
        lru_in_weight, lru_gate_weight, conv_weight = (
            jnp.pad(w, ((0, 0), (0, extra * size))) for w in (lru_in_weight, lru_gate_weight, conv_weight)
        )
        gate_a_weight, gate_x_weight = (
            jnp.pad(w, ((0, extra), (0, 0), (0, 0))) for w in (gate_a_weight, gate_x_weight)
        )
        decay_param = jnp.pad(decay_param, (0, extra * size))
        mix_out_weight = jnp.pad(mix_out_weight, ((0, extra * size), (0, 0)))
    cs = lru_in_weight.shape[1] // PAIR

    small = [
        tokens,
        ffn1_gain[None],
        mix_gain[None],
        ffn2_gain[None],
        conv_weight,
        gate_a_weight,
        gate_x_weight,
        jax.nn.softplus(-decay_param)[None],
    ]
    big = [
        ffn1_gate,
        ffn1_up,
        ffn1_down.reshape(PAIR, hs, dn),
        lru_in_weight,
        lru_gate_weight,
        mix_out_weight.reshape(PAIR, cs, dn),
        ffn2_gate,
        ffn2_up,
        ffn2_down.reshape(PAIR, hs, dn),
    ]
    bf16, f32 = jnp.bfloat16, jnp.float32
    sem = pltpu.SemaphoreType.DMA
    scratch = [
        pltpu.VMEM((MATS, n, hs, dn), bf16),
        pltpu.VMEM((MATS, n, cs, dn), bf16),
        pltpu.VMEM((MATS, n, hs, dn), bf16),
        pltpu.VMEM((MATS, hs, dn), bf16),
        pltpu.VMEM((MATS, cs, dn), bf16),
        pltpu.VMEM((MATS, hs, dn), bf16),
        pltpu.VMEM((3, chips, CORES, n, r, dn), bf16),
        pltpu.VMEM((n, chips, r, dn), bf16),
        pltpu.VMEM((n, chips, r, dn), bf16),
        pltpu.VMEM((n, nx - 1, PAIR, r, dn), bf16),
        pltpu.VMEM((n, nx - 1, PAIR, r, dn), bf16),
        pltpu.VMEM((n, r, dn), bf16),
        pltpu.VMEM((n, r, dn), bf16),
        pltpu.VMEM((n, PAIR, r, dn), f32),
        pltpu.VMEM((2, chips, r, dn), f32),
        pltpu.VMEM((CORES, chips * r, hs), bf16),
        pltpu.VMEM((CORES + 1, chips * r, hs), f32),
        pltpu.VMEM((CORES, chips * r, cs), bf16),
        pltpu.VMEM((MATS - 1, CORES * chips * r, cs), f32),
        pltpu.VMEM((n, r, dn), bf16),
        pltpu.VMEM((n, r, dn), bf16),
        *[pltpu.VMEM((MATS - 1, dn, PAIR * u), bf16) for u in (hs, cs, hs)],
        *[pltpu.VMEM((MATS - 1, PAIR, u, dn), bf16) for u in (hs, cs, hs)],
        pltpu.VMEM((cs, cs), f32),
        pltpu.VMEM((cs, cs), f32),
        sem((3, MATS, n)),
        sem((3, MATS)),
        sem((3, MATS, 2 * nz)),
        sem((3, MATS, nz, ny)),
        sem((3, MATS)),
        sem((3, chips, CORES, parts)),
        sem((3, 4 * nx, parts)),
        sem((3, n)),
        sem((3, n)),
        sem((3, n, nx - 1)),
        sem((3, n, nx - 1)),
        sem((3, n)),
        sem((3, n)),
        sem((3, MATS)),
    ]
    vmem = pl.BlockSpec(memory_space=pltpu.VMEM)
    hbm = pl.BlockSpec(memory_space=pl.ANY)
    result = pl.pallas_call(
        functools.partial(layer_kernel, n, t),
        out_shape=jax.ShapeDtypeStruct((n, r, dn), bf16),
        in_specs=[vmem] * len(small) + [hbm] * len(big),
        out_specs=vmem,
        scratch_shapes=scratch,
        compiler_params=pltpu.CompilerParams(
            collective_id=0, has_side_effects=True, vmem_limit_bytes=66_000_000
        ),
    )(*small, *big)
    return result.transpose(1, 0, 2).reshape(r, width)


def solution(mesh):
    n, t = mesh.shape["fs"], mesh.shape["tp"]
    in_specs = (
        P(("fs", "tp"), None),
        P(),
        P("fs", "tp"),
        P("fs", "tp"),
        P("tp", "fs"),
        P(),
        P("fs", "tp"),
        P("fs", "tp"),
        P(None, "tp"),
        P("tp", None, None),
        P("tp", None, None),
        P("tp"),
        P("tp", "fs"),
        P(),
        P("fs", "tp"),
        P("fs", "tp"),
        P("tp", "fs"),
    )

    def run(*args):
        return body(n, t, *args)

    return jax.shard_map(
        run, mesh=mesh, in_specs=in_specs, out_specs=P(("fs", "tp"), None), check_vma=False
    )
```

```python
import functools
import math

import jax
import jax.numpy as jnp
from jax import lax
from jax.experimental import pallas as pl
from jax.experimental.pallas import tpu as pltpu
from jax.sharding import PartitionSpec as P

EPS = 1e-06
CORES = 2
PAIR = 2
MATS = 3
ROW_PARTS = 4
MESH = pl.DeviceIdType.MESH


def dot_nt(a, b):
    return lax.dot_general(a, b, (((1,), (1,)), ((), ())), preferred_element_type=jnp.float32)


def sigmoid(v):
    return 1.0 / (1.0 + jnp.exp(-v))


def shift_down(values, step, fill):
    pad = jnp.full((step, values.shape[1]), fill, values.dtype)
    return jnp.concatenate([pad, values[: values.shape[0] - step]], axis=0)


class Place:
    def __init__(self, n, t):
        self.n, self.t = n, t
        self.ny = math.isqrt(n // PAIR)
        self.nz = n // self.ny
        self.nq = self.nz // PAIR
        self.nx = t // CORES
        fs, tp = lax.axis_index("fs"), lax.axis_index("tp")
        self.fs, self.tp = fs, tp
        self.z, self.y = fs // self.ny, fs % self.ny
        self.q, self.zp = self.z // PAIR, self.z % PAIR
        self.x, self.c = tp // CORES, tp % CORES
        self.chips = PAIR * self.nx
        self.inner = (self.q + self.zp) % PAIR

    def z_at(self, i):
        q = (self.q + i // PAIR) % self.nq
        turn = self.inner * (1 if i >= PAIR else 0) if isinstance(i, int) else jnp.where(i >= PAIR, self.inner, 0)
        return q * PAIR + (self.zp + i + turn) % PAIR

    def f_at(self, i, j):
        return self.z_at(i) * self.ny + (self.y + j) % self.ny

    def at_z(self, z):
        return (z * self.ny + self.y, self.tp)

    def at_y(self, j):
        return (self.z * self.ny + (self.y + j) % self.ny, self.tp)

    def at_x(self, s):
        return (self.fs, ((self.x + s) % self.nx) * CORES + self.c)

    def other_z(self):
        return self.at_z(self.q * PAIR + 1 - self.zp)

    def other_core(self):
        return (self.fs, self.x * CORES + 1 - self.c)


def remote(src, dst, send, recv, device):
    return pltpu.make_async_remote_copy(
        src_ref=src, dst_ref=dst, send_sem=send, recv_sem=recv, device_id=device, device_id_type=MESH
    )


def layer_kernel(n, t, *refs):
    (tokens_in, gain1, gainm, gain2, taps, gate_a, gate_x, slope) = refs[:8]
    raw = (refs[8:11], refs[11:14], refs[14:17])
    out = refs[17]
    (w1, wm, w2, rel1, relm, rel2, rows_of, xs, xr, ys, yr, zs, zr, own, part_sum, hid, acc, hid_m, acc_m, res, tokens, load1, loadm, load2, flip1, flipm, flip2, wide_a, wide_x) = refs[18:47]
    (rw, rrel, zsend, ysend, lsem, gr, gs, xss, xsr, yss, ysr, zss, zsr, load_sem) = refs[47:]
    weights = (w1, wm, w2)
    relays = (rel1, relm, rel2)
    me = Place(n, t)
    r, width = tokens_in.shape
    dn = width // n
    loads, flips = (load1, loadm, load2), (flip1, flipm, flip2)
    sources = [
        [flips[s].at[k] for k in range(MATS - 1)]
        + [raw[s][MATS - 1]]
        for s in range(3)
    ]

    def load(s, k):
        return pltpu.make_async_copy(raw[s][k], loads[s].at[k], load_sem.at[s, k])

    def flip(s, k):
        load(s, k).wait()
        flips[s][k] = loads[s][k].T.reshape(flips[s].shape[1:])

    for s in range(3):
        for k in range(MATS - 1):
            load(s, k).start()
    chips, nx, ny, nz = me.chips, me.nx, me.ny, me.nz
    parts = math.gcd(n, ROW_PARTS)
    step = n // parts
    mine = me.zp * nx + me.x
    rest = (1 - me.zp) * nx + me.x

    barrier = pltpu.get_barrier_semaphore()
    peers = [me.at_z((me.z + d) % nz) for d in range(1, nz)]
    peers += [me.at_y(j) for j in range(1, ny)]
    peers += [me.at_x(s) for s in range(1, nx)]
    peers += [me.other_core()]
    for peer in peers:
        pl.semaphore_signal(barrier, inc=1, device_id=peer, device_id_type=MESH)
    flip(0, 0)
    for f in range(n):
        tokens[f] = tokens_in[:, f * dn : (f + 1) * dn]
    pl.semaphore_wait(barrier, len(peers))

    def z_piece(s, k, i):
        z = me.z_at(i)
        return remote(
            sources[s][k].at[z % PAIR],
            weights[s].at[k, me.fs],
            zsend.at[s, k, i],
            rw.at[s, k, me.fs],
            me.at_z(z),
        )

    def y_piece(s, k, i, j):
        f = me.f_at(i, 0)
        src = sources[s][k].at[me.zp] if isinstance(i, int) and i == 0 else weights[s].at[k, f]
        return remote(
            src, weights[s].at[k, f], ysend.at[s, k, i, j], rw.at[s, k, f], me.at_y(j)
        )

    def local_piece(s, k):
        return pltpu.make_async_copy(
            sources[s][k].at[me.zp], weights[s].at[k, me.fs], lsem.at[s, k]
        )

    def arrived(s, k, f):
        place = weights[s].at[k, f]
        remote(place, place, zsend.at[s, k, 0], rw.at[s, k, f], me.at_y(0)).wait_recv()

    def relay_in(s, k):
        return remote(
            sources[s][k].at[me.zp],
            relays[s].at[k],
            zsend.at[s, k, 0],
            rrel.at[s, k],
            me.other_z(),
        )

    def relay_near(s, k, i):
        f = me.f_at(1, 0)
        place = weights[s].at[k, f]
        return remote(place, place, zsend.at[s, k, nz + i], rw.at[s, k, f], me.at_z(me.z_at(i)))

    def relay_out(s, k, i):
        f = me.f_at(1, 0)
        return remote(
            relays[s].at[k],
            weights[s].at[k, f],
            zsend.at[s, k, nz + i],
            rw.at[s, k, f],
            me.at_z(me.z_at(i)),
        )

    def when_inner(*actions):
        @pl.when(me.inner == 1)
        def _():
            for act, s, k in actions:
                act(s, k)

    def when_end(*actions):
        @pl.when(me.inner == 0)
        def _():
            for act, s, k in actions:
                act(s, k)

    def to_inner(s, k):
        for i in range(PAIR, nz, 2):
            z_piece(s, k, i).start()

    def to_end(s, k):
        for i in range(PAIR + 1, nz, 2):
            z_piece(s, k, i).start()

    def send_near(s, k):
        z_piece(s, k, 1).start()

    def send_both(s, k):
        send_near(s, k)
        relay_in(s, k).start()

    def relay(s, k):
        relay_in(s, k).wait_recv()
        for i in range(PAIR, nz, 2):
            relay_out(s, k, i).start()

    def send_own(s, k):
        for j in range(1, ny):
            y_piece(s, k, 0, j).start()
        local_piece(s, k).start()

    def forward(s, k, i):
        arrived(s, k, me.f_at(i, 0))
        for j in range(1, ny):
            y_piece(s, k, i, j).start()
        if i == 1:

            @pl.when(me.inner == 1)
            def _():
                for m in range(PAIR + 1, nz, 2):
                    relay_near(s, k, m).start()

    def collect(s, k):
        local_piece(s, k).wait()
        for i in range(nz):
            for j in range(1, ny):
                arrived(s, k, me.f_at(i, j))

    def row_copy(g, p, c, slot, part, device):
        block = rows_of.at[g, p, c, pl.ds(part * step, step)]
        return remote(block, block, gs.at[g, slot, part], gr.at[g, p, c, part], device)

    def row_wait(g, p, c, part):
        row_copy(g, p, c, 0, part, me.other_core()).wait_recv()

    def norm_rows(values, gain):
        total = jnp.zeros((r, 1), jnp.float32)
        for f in range(n):
            wide = values(f)
            total += jnp.sum(wide * wide, axis=-1, keepdims=True)
        scale = lax.rsqrt(total / width + EPS)
        return lambda f: (values(f) * scale * gain[:, f * dn : (f + 1) * dn]).astype(jnp.bfloat16)

    row_sends = []

    def send_rows(g, values, gain):
        normed = norm_rows(values, gain)
        for f in range(n):
            rows_of[g, mine, me.c, f] = normed(f)
        targets = [me.other_z()] + [me.at_x(d) for d in range(1, nx)] + [me.other_core()]
        for slot, device in enumerate(targets):
            for part in range(parts):
                copy = row_copy(g, mine, me.c, slot, part, device)
                copy.start()
                row_sends.append(copy)

    def spread(g, p, slot, part, across):
        row_wait(g, p, me.c, part)
        targets = [me.at_x(d) for d in range(1, nx)] if across else []
        targets += [me.other_core()]
        for m, device in enumerate(targets):
            copy = row_copy(g, p, me.c, slot + m, part, device)
            copy.start()
            row_sends.append(copy)

    def near_rows(g):
        for part in range(parts):
            spread(g, rest, nx + 1, part, True)

    def far_rows(g):
        slot = 2 * nx + 1
        for base in (me.zp * nx, (1 - me.zp) * nx):
            for d in range(1, nx):
                for part in range(parts):
                    spread(g, base + (me.x + d) % nx, slot, part, False)
                slot += 1
        for p in range(chips):
            for part in range(parts):
                row_wait(g, p, 1 - me.c, part)

    def core_part(g, f):
        return remote(xs.at[f], xr.at[f], xss.at[g, f], xsr.at[g, f], me.other_core())

    def x_part(g, f, s):
        return remote(
            ys.at[f, s - 1], yr.at[f, s - 1], yss.at[g, f, s - 1], ysr.at[g, f, s - 1], me.at_x(s)
        )

    def z_part(g, f):
        return remote(zs.at[f], zr.at[f], zss.at[g, f], zsr.at[g, f], me.other_z())

    order = [(0, 0)]
    for i in range(1, nz + 1):
        order += [(i, 0)] if i < nz else []
        order += [(i - 1, j) for j in range(1, ny)]

    def reduce_rows(g, s, hidden, early=(), paced=False):
        last = MATS - 1

        def begin(m):
            i, j = order[m]
            f = me.f_at(i, j)
            if j:
                arrived(s, last, f)
            elif i == 0:
                local_piece(s, last).wait()
            elif i not in early:
                forward(s, last, i)
            weight = weights[s][last, f]
            term = jnp.dot(hidden[1 - me.c], weight, preferred_element_type=jnp.float32)
            xs[f] = term.astype(jnp.bfloat16).reshape(chips, r, dn)
            core_part(g, f).start()
            term = jnp.dot(hidden[me.c], weight, preferred_element_type=jnp.float32)
            part_sum[m % 2] = term.reshape(chips, r, dn)

        def cross(m):
            f = me.f_at(*order[m])
            core_part(g, f).wait_recv()
            for h in range(PAIR):
                for d in range(1, nx):
                    p = h * nx + (me.x + d) % nx
                    total = part_sum[m % 2, p] + xr[f, p].astype(jnp.float32)
                    ys[f, d - 1, h] = total.astype(jnp.bfloat16)
            for d in range(1, nx):
                x_part(g, f, d).start()
            for h in range(PAIR):
                p = h * nx + me.x
                own[f, h] = part_sum[m % 2, p] + xr[f, p].astype(jnp.float32)

        def pass_on(m):
            f = me.f_at(*order[m])
            total = own[f, 1 - me.zp]
            for d in range(1, nx):
                x_part(g, f, d).wait_recv()
                total = total + yr[f, d - 1, 1 - me.zp].astype(jnp.float32)
            zs[f] = total.astype(jnp.bfloat16)
            z_part(g, f).start()

        for m in range(n + 3):
            if paced and 1 <= m <= n:
                cross(m - 1)
            if m < n:
                begin(m)
            if not paced and 1 <= m <= n:
                cross(m - 1)
            if m >= 3:
                pass_on(m - 3)

    def reduced(g, f):
        z_part(g, f).wait_recv()
        total = own[f, me.zp]
        for d in range(1, nx):
            total = total + yr[f, d - 1, me.zp].astype(jnp.float32)
        return total + zr[f].astype(jnp.float32)

    def drain(g):
        def one(f, carry):
            core_part(g, f).wait_send()
            for d in range(1, nx):
                x_part(g, f, d).wait_send()
            z_part(g, f).wait_send()
            return carry

        lax.fori_loop(0, n, one, 0)

    def project(g, s, k, c, to):
        acc[to] = jnp.zeros_like(acc[to])

        def feature(f, carry):
            rows = rows_of[g, :, c, f].reshape(chips * r, dn)
            acc[to] += dot_nt(rows, weights[s][k, f])
            return carry

        lax.fori_loop(0, n, feature, 0)

    def gate_rows(g, s):
        def side(c, carry):
            project(g, s, 0, c, c)
            return carry

        lax.fori_loop(0, CORES, side, 0)

    def hidden_rows(g, s, between=()):
        for c in (1 - me.c, me.c):
            project(g, s, 1, c, CORES)
            gate = acc[c]
            hid[c] = (gate * sigmoid(gate) * acc[CORES]).astype(jnp.bfloat16)
            forward_all(s, MATS - 1, between)
            between = ()

    def mix_rows(g, s):
        acc_m[...] = jnp.zeros_like(acc_m)
        length = nx * CORES * r

        def feature(f, carry):
            rows = rows_of[g, :, :, f].reshape(PAIR * length, dn)
            for k in range(MATS - 1):
                acc_m[k] += dot_nt(rows, weights[s][k, f])
            return carry

        lax.fori_loop(0, n, feature, 0)
        channels = taps.shape[1] // PAIR

        def mine_of(v):
            return jnp.where(me.zp == 0, v[:, :channels], v[:, channels:])

        tap = mine_of(taps[...].astype(jnp.float32))
        fall = mine_of(slope[...])
        count, size = gate_a.shape[0] // PAIR, gate_a.shape[1]
        for wide, gate in ((wide_a, gate_a), (wide_x, gate_x)):
            wide[...] = jnp.zeros_like(wide)
            for m in range(count):
                at = slice(m * size, (m + 1) * size)
                wide[at, at] = gate[me.zp * count + m].astype(jnp.float32)
        a, b = wide_a[...].astype(jnp.bfloat16), wide_x[...].astype(jnp.bfloat16)
        for q in range(PAIR):
            rows = pl.ds(q * length, length)
            lru = acc_m[0, rows].astype(jnp.bfloat16).astype(jnp.float32)
            gated = acc_m[1, rows].astype(jnp.bfloat16).astype(jnp.float32)
            conv = tap[0:1] * lru
            for k in range(1, tap.shape[0]):
                conv = conv + tap[k : k + 1] * shift_down(lru, k, 0.0)
            low = conv.astype(jnp.bfloat16)
            recall = sigmoid(jnp.dot(low, a, preferred_element_type=jnp.float32))
            admit = sigmoid(jnp.dot(low, b, preferred_element_type=jnp.float32))
            log_keep = -8.0 * recall * fall
            keep = jnp.exp(log_keep)
            grow = -jnp.tanh(log_keep) * (1.0 + keep * keep)
            state = jnp.sqrt(grow) * admit * low.astype(jnp.float32)
            step = 1
            while step < length:
                state = state + keep * shift_down(state, step, 0.0)
                keep = keep * shift_down(keep, step, 1.0)
                step *= 2
            inner = 0.7978845608028654 * (gated + 0.044715 * gated * gated * gated)
            mixed = state * (0.5 * gated * (1.0 + jnp.tanh(inner)))
            mixed = mixed.astype(jnp.bfloat16)
            for x in range(nx):
                for c in range(CORES):
                    at = (x * CORES + c) * r
                    hid_m[c, pl.ds((q * nx + x) * r, r)] = mixed[at : at + r]

    first = range(PAIR, nz, PAIR)
    second = range(PAIR + 1, nz, PAIR)

    def forward_all(s, k, which):
        for i in which:
            forward(s, k, i)

    def take_near(s, k):
        forward(s, k, 1)

    when_end((send_both, 0, 0))
    when_inner((send_near, 0, 0), (to_inner, 0, 0))
    send_own(0, 0)
    send_rows(0, lambda f: tokens[f].astype(jnp.float32), gain1)
    flip(0, 1)
    when_end((send_both, 0, 1), (send_both, 0, 2))
    when_inner((send_near, 0, 1), (to_inner, 0, 1), (to_end, 0, 0), (send_near, 0, 2))
    send_own(0, 1)
    for s in (1, 2):
        for k in range(MATS - 1):
            flip(s, k)
    take_near(0, 0)
    when_inner((relay, 0, 0), (to_end, 0, 1))
    near_rows(0)
    forward_all(0, 0, first)
    far_rows(0)
    when_inner((take_near, 0, 1), (relay, 0, 1), (to_inner, 0, 2), (to_end, 0, 2))
    forward_all(0, 0, second)
    when_end((take_near, 0, 1))
    forward_all(0, 1, first)
    collect(0, 0)
    when_end(*[(send_both, 1, k) for k in range(MATS)], (send_both, 2, 0), (send_both, 2, 1))
    gate_rows(0, 0)
    forward_all(0, 1, second)
    send_own(0, 2)
    take_near(0, 2)
    when_inner((relay, 0, 2))
    when_inner(*[(act, 1, k) for k in range(MATS) for act in (send_near, to_inner, to_end, relay)])
    collect(0, 1)
    when_inner(*[(take_near, 1, k) for k in range(MATS)])
    when_inner((send_near, 2, 0), (send_near, 2, 1), (to_inner, 2, 0), (to_inner, 2, 1))
    hidden_rows(0, 0)
    reduce_rows(0, 0, hid, [1], True)
    when_end(*[(take_near, 1, k) for k in range(MATS)])
    for k in range(MATS):
        send_own(1, k)
    send_own(2, 0)
    for f in range(n):
        res[f] = (tokens[f].astype(jnp.float32) + 0.5 * reduced(0, f)).astype(jnp.bfloat16)
    send_rows(1, lambda f: res[f].astype(jnp.float32), gainm)
    when_end((send_both, 2, 2))
    for k in range(MATS):
        forward_all(1, k, range(2, nz))
    when_end((take_near, 2, 0), (take_near, 2, 1))
    near_rows(1)
    when_inner((to_end, 2, 0), (take_near, 2, 0), (to_end, 2, 1), (take_near, 2, 1))
    when_inner((relay, 2, 0), (relay, 2, 1), (to_inner, 2, 2))
    when_inner((send_near, 2, 2))
    send_own(2, 1)
    far_rows(1)
    for k in range(MATS - 1):
        collect(1, k)
    mix_rows(1, 1)
    forward_all(2, 0, first)
    drain(0)
    reduce_rows(1, 1, hid_m, range(1, nz))
    forward_all(2, 1, first)
    for f in range(n):
        res[f] = (res[f].astype(jnp.float32) + reduced(1, f)).astype(jnp.bfloat16)
    send_rows(2, lambda f: res[f].astype(jnp.float32), gain2)
    forward_all(2, 0, second)
    near_rows(2)
    when_inner((to_end, 2, 2), (relay, 2, 2))
    take_near(2, 2)
    forward_all(2, 1, second)
    send_own(2, 2)
    far_rows(2)
    collect(2, 0)
    gate_rows(2, 2)
    collect(2, 1)
    hidden_rows(2, 2, first)
    drain(1)
    reduce_rows(2, 2, hid, [1, *first], True)
    for f in range(n):
        out[f] = (res[f].astype(jnp.float32) + 0.5 * reduced(2, f)).astype(jnp.bfloat16)

    for copy in row_sends:
        copy.wait_send()
    for s in range(3):
        for k in range(MATS):
            z_piece(s, k, 1).wait_send()
            for i in range(nz):
                for j in range(1, ny):
                    y_piece(s, k, i, j).wait_send()

    def finish_inner(s, k):
        for i in range(PAIR, nz):
            z_piece(s, k, i).wait_send()
            (relay_near if i % PAIR else relay_out)(s, k, i).wait_send()

    def finish_end(s, k):
        relay_in(s, k).wait_send()

    when_inner(*[(finish_inner, s, k) for s in range(3) for k in range(MATS)])
    when_end(*[(finish_end, s, k) for s in range(3) for k in range(MATS)])

    drain(2)


def body(
    n,
    t,
    tokens,
    ffn1_gain,
    ffn1_gate,
    ffn1_up,
    ffn1_down,
    mix_gain,
    lru_in_weight,
    lru_gate_weight,
    conv_weight,
    gate_a_weight,
    gate_x_weight,
    decay_param,
    mix_out_weight,
    ffn2_gain,
    ffn2_gate,
    ffn2_up,
    ffn2_down,
):
    r, width = tokens.shape
    dn = width // n
    ny = math.isqrt(n // PAIR)
    nz, nx = n // ny, t // CORES
    chips = PAIR * nx
    parts = math.gcd(n, ROW_PARTS)
    hs = ffn1_gate.shape[1] // PAIR
    size = gate_a_weight.shape[1]
    extra = -gate_a_weight.shape[0] % PAIR
    if extra:
        lru_in_weight, lru_gate_weight, conv_weight = (
            jnp.pad(w, ((0, 0), (0, extra * size))) for w in (lru_in_weight, lru_gate_weight, conv_weight)
        )
        gate_a_weight, gate_x_weight = (
            jnp.pad(w, ((0, extra), (0, 0), (0, 0))) for w in (gate_a_weight, gate_x_weight)
        )
        decay_param = jnp.pad(decay_param, (0, extra * size))
        mix_out_weight = jnp.pad(mix_out_weight, ((0, extra * size), (0, 0)))
    cs = lru_in_weight.shape[1] // PAIR

    small = [
        tokens,
        ffn1_gain[None],
        mix_gain[None],
        ffn2_gain[None],
        conv_weight,
        gate_a_weight,
        gate_x_weight,
        jax.nn.softplus(-decay_param)[None],
    ]
    big = [
        ffn1_gate,
        ffn1_up,
        ffn1_down.reshape(PAIR, hs, dn),
        lru_in_weight,
        lru_gate_weight,
        mix_out_weight.reshape(PAIR, cs, dn),
        ffn2_gate,
        ffn2_up,
        ffn2_down.reshape(PAIR, hs, dn),
    ]
    bf16, f32 = jnp.bfloat16, jnp.float32
    sem = pltpu.SemaphoreType.DMA
    scratch = [
        pltpu.VMEM((MATS, n, hs, dn), bf16),
        pltpu.VMEM((MATS, n, cs, dn), bf16),
        pltpu.VMEM((MATS, n, hs, dn), bf16),
        pltpu.VMEM((MATS, hs, dn), bf16),
        pltpu.VMEM((MATS, cs, dn), bf16),
        pltpu.VMEM((MATS, hs, dn), bf16),
        pltpu.VMEM((3, chips, CORES, n, r, dn), bf16),
        pltpu.VMEM((n, chips, r, dn), bf16),
        pltpu.VMEM((n, chips, r, dn), bf16),
        pltpu.VMEM((n, nx - 1, PAIR, r, dn), bf16),
        pltpu.VMEM((n, nx - 1, PAIR, r, dn), bf16),
        pltpu.VMEM((n, r, dn), bf16),
        pltpu.VMEM((n, r, dn), bf16),
        pltpu.VMEM((n, PAIR, r, dn), f32),
        pltpu.VMEM((2, chips, r, dn), f32),
        pltpu.VMEM((CORES, chips * r, hs), bf16),
        pltpu.VMEM((CORES + 1, chips * r, hs), f32),
        pltpu.VMEM((CORES, chips * r, cs), bf16),
        pltpu.VMEM((MATS - 1, CORES * chips * r, cs), f32),
        pltpu.VMEM((n, r, dn), bf16),
        pltpu.VMEM((n, r, dn), bf16),
        *[pltpu.VMEM((MATS - 1, dn, PAIR * u), bf16) for u in (hs, cs, hs)],
        *[pltpu.VMEM((MATS - 1, PAIR, u, dn), bf16) for u in (hs, cs, hs)],
        pltpu.VMEM((cs, cs), f32),
        pltpu.VMEM((cs, cs), f32),
        sem((3, MATS, n)),
        sem((3, MATS)),
        sem((3, MATS, 2 * nz)),
        sem((3, MATS, nz, ny)),
        sem((3, MATS)),
        sem((3, chips, CORES, parts)),
        sem((3, 4 * nx, parts)),
        sem((3, n)),
        sem((3, n)),
        sem((3, n, nx - 1)),
        sem((3, n, nx - 1)),
        sem((3, n)),
        sem((3, n)),
        sem((3, MATS)),
    ]
    vmem = pl.BlockSpec(memory_space=pltpu.VMEM)
    hbm = pl.BlockSpec(memory_space=pl.ANY)
    result = pl.pallas_call(
        functools.partial(layer_kernel, n, t),
        out_shape=jax.ShapeDtypeStruct((n, r, dn), bf16),
        in_specs=[vmem] * len(small) + [hbm] * len(big),
        out_specs=vmem,
        scratch_shapes=scratch,
        compiler_params=pltpu.CompilerParams(
            collective_id=0, has_side_effects=True, vmem_limit_bytes=66_000_000
        ),
    )(*small, *big)
    return result.transpose(1, 0, 2).reshape(r, width)


def solution(mesh):
    n, t = mesh.shape["fs"], mesh.shape["tp"]
    in_specs = (
        P(("fs", "tp"), None),
        P(),
        P("fs", "tp"),
        P("fs", "tp"),
        P("tp", "fs"),
        P(),
        P("fs", "tp"),
        P("fs", "tp"),
        P(None, "tp"),
        P("tp", None, None),
        P("tp", None, None),
        P("tp"),
        P("tp", "fs"),
        P(),
        P("fs", "tp"),
        P("fs", "tp"),
        P("tp", "fs"),
    )

    def run(*args):
        return body(n, t, *args)

    return jax.shard_map(
        run, mesh=mesh, in_specs=in_specs, out_specs=P(("fs", "tp"), None), check_vma=False
    )
```

```python
import functools
import math

import jax
import jax.numpy as jnp
from jax import lax
from jax.experimental import pallas as pl
from jax.experimental.pallas import tpu as pltpu
from jax.sharding import PartitionSpec as P

EPS = 1e-06
CORES = 2
PAIR = 2
MATS = 3
ROW_PARTS = 4
LANES = 128
MESH = pl.DeviceIdType.MESH


def dot_nt(a, b):
    return lax.dot_general(a, b, (((1,), (1,)), ((), ())), preferred_element_type=jnp.float32)


def sigmoid(v):
    return 1.0 / (1.0 + jnp.exp(-v))


def shift_down(values, step, fill):
    pad = jnp.full((step, values.shape[1]), fill, values.dtype)
    return jnp.concatenate([pad, values[: values.shape[0] - step]], axis=0)


class Place:
    def __init__(self, n, t):
        self.n, self.t = n, t
        self.ny = math.isqrt(n // PAIR)
        self.nz = n // self.ny
        self.nq = self.nz // PAIR
        self.nx = t // CORES
        fs, tp = lax.axis_index("fs"), lax.axis_index("tp")
        self.fs, self.tp = fs, tp
        self.z, self.y = fs // self.ny, fs % self.ny
        self.q, self.zp = self.z // PAIR, self.z % PAIR
        self.x, self.c = tp // CORES, tp % CORES
        self.chips = PAIR * self.nx
        self.inner = (self.q + self.zp) % PAIR

    def z_at(self, i):
        q = (self.q + i // PAIR) % self.nq
        turn = self.inner * (1 if i >= PAIR else 0) if isinstance(i, int) else jnp.where(i >= PAIR, self.inner, 0)
        return q * PAIR + (self.zp + i + turn) % PAIR

    def f_at(self, i, j):
        return self.z_at(i) * self.ny + (self.y + j) % self.ny

    def at_z(self, z):
        return (z * self.ny + self.y, self.tp)

    def at_y(self, j):
        return (self.z * self.ny + (self.y + j) % self.ny, self.tp)

    def at_x(self, s):
        return (self.fs, ((self.x + s) % self.nx) * CORES + self.c)

    def other_z(self):
        return self.at_z(self.q * PAIR + 1 - self.zp)

    def other_core(self):
        return (self.fs, self.x * CORES + 1 - self.c)


def remote(src, dst, send, recv, device):
    return pltpu.make_async_remote_copy(
        src_ref=src, dst_ref=dst, send_sem=send, recv_sem=recv, device_id=device, device_id_type=MESH
    )


def layer_kernel(n, t, *refs):
    (tokens_in, gain1, gainm, gain2, taps, gate_a, gate_x, slope) = refs[:8]
    raw = (refs[8:11], refs[11:14], refs[14:17])
    out = refs[17]
    (w1, wm, w2, rel1, relm, rel2, rows_of, xs, xr, ys, yr, zs, zr, own, part_sum, hid, acc, hid_m, acc_m, res, tokens, load1, loadm, load2, flip1, flipm, flip2, wide_a, wide_x) = refs[18:47]
    (rw, rrel, zsend, ysend, lsem, gr, gs, xss, xsr, yss, ysr, zss, zsr, load_sem) = refs[47:]
    weights = (w1, wm, w2)
    relays = (rel1, relm, rel2)
    me = Place(n, t)
    r, width = tokens_in.shape
    dn = width // n
    loads, flips = (load1, loadm, load2), (flip1, flipm, flip2)
    sources = [
        [flips[s].at[k] for k in range(MATS - 1)]
        + [raw[s][MATS - 1]]
        for s in range(3)
    ]

    def load(s, k):
        return pltpu.make_async_copy(raw[s][k], loads[s].at[k], load_sem.at[s, k])

    def flip(s, k):
        load(s, k).wait()
        flips[s][k] = loads[s][k].T.reshape(flips[s].shape[1:])

    for s in range(3):
        for k in range(MATS - 1):
            load(s, k).start()
    chips, nx, ny, nz = me.chips, me.nx, me.ny, me.nz
    parts = math.gcd(n, ROW_PARTS)
    step = n // parts
    group = 1 if dn % LANES else math.gcd(n, 4)
    mine = me.zp * nx + me.x
    rest = (1 - me.zp) * nx + me.x

    barrier = pltpu.get_barrier_semaphore()
    peers = [me.at_z((me.z + d) % nz) for d in range(1, nz)]
    peers += [me.at_y(j) for j in range(1, ny)]
    peers += [me.at_x(s) for s in range(1, nx)]
    peers += [me.other_core()]
    for peer in peers:
        pl.semaphore_signal(barrier, inc=1, device_id=peer, device_id_type=MESH)
    flip(0, 0)
    for f in range(n):
        tokens[f] = tokens_in[:, f * dn : (f + 1) * dn]
    pl.semaphore_wait(barrier, len(peers))

    def z_piece(s, k, i):
        z = me.z_at(i)
        return remote(
            sources[s][k].at[z % PAIR],
            weights[s].at[k, me.fs],
            zsend.at[s, k, i],
            rw.at[s, k, me.fs],
            me.at_z(z),
        )

    def y_piece(s, k, i, j):
        f = me.f_at(i, 0)
        src = sources[s][k].at[me.zp] if isinstance(i, int) and i == 0 else weights[s].at[k, f]
        return remote(
            src, weights[s].at[k, f], ysend.at[s, k, i, j], rw.at[s, k, f], me.at_y(j)
        )

    def local_piece(s, k):
        return pltpu.make_async_copy(
            sources[s][k].at[me.zp], weights[s].at[k, me.fs], lsem.at[s, k]
        )

    def arrived(s, k, f):
        place = weights[s].at[k, f]
        remote(place, place, zsend.at[s, k, 0], rw.at[s, k, f], me.at_y(0)).wait_recv()

    def relay_in(s, k):
        return remote(
            sources[s][k].at[me.zp],
            relays[s].at[k],
            zsend.at[s, k, 0],
            rrel.at[s, k],
            me.other_z(),
        )

    def relay_near(s, k, i):
        f = me.f_at(1, 0)
        place = weights[s].at[k, f]
        return remote(place, place, zsend.at[s, k, nz + i], rw.at[s, k, f], me.at_z(me.z_at(i)))

    def relay_out(s, k, i):
        f = me.f_at(1, 0)
        return remote(
            relays[s].at[k],
            weights[s].at[k, f],
            zsend.at[s, k, nz + i],
            rw.at[s, k, f],
            me.at_z(me.z_at(i)),
        )

    def when_inner(*actions):
        @pl.when(me.inner == 1)
        def _():
            for act, s, k in actions:
                act(s, k)

    def when_end(*actions):
        @pl.when(me.inner == 0)
        def _():
            for act, s, k in actions:
                act(s, k)

    def to_inner(s, k):
        for i in range(PAIR, nz, 2):
            z_piece(s, k, i).start()

    def to_end(s, k):
        for i in range(PAIR + 1, nz, 2):
            z_piece(s, k, i).start()

    def send_near(s, k):
        z_piece(s, k, 1).start()

    def send_both(s, k):
        send_near(s, k)
        relay_in(s, k).start()

    def relay(s, k):
        relay_in(s, k).wait_recv()
        for i in range(PAIR, nz, 2):
            relay_out(s, k, i).start()

    def send_own(s, k):
        for j in range(1, ny):
            y_piece(s, k, 0, j).start()
        local_piece(s, k).start()

    def forward(s, k, i):
        arrived(s, k, me.f_at(i, 0))
        for j in range(1, ny):
            y_piece(s, k, i, j).start()
        if i == 1:

            @pl.when(me.inner == 1)
            def _():
                for m in range(PAIR + 1, nz, 2):
                    relay_near(s, k, m).start()

    def collect(s, k):
        local_piece(s, k).wait()
        for i in range(nz):
            for j in range(1, ny):
                arrived(s, k, me.f_at(i, j))

    def row_copy(g, p, c, slot, part, device):
        block = rows_of.at[g, p, c, pl.ds(part * step, step)]
        return remote(block, block, gs.at[g, slot, part], gr.at[g, p, c, part], device)

    def row_wait(g, p, c, part):
        row_copy(g, p, c, 0, part, me.other_core()).wait_recv()

    def norm_rows(values, gain):
        total = jnp.zeros((r, 1), jnp.float32)
        for f in range(n):
            wide = values(f)
            total += jnp.sum(wide * wide, axis=-1, keepdims=True)
        scale = lax.rsqrt(total / width + EPS)
        return lambda f: (values(f) * scale * gain[:, f * dn : (f + 1) * dn]).astype(jnp.bfloat16)

    row_sends = []

    def send_rows(g, values, gain):
        normed = norm_rows(values, gain)
        for f in range(n):
            rows_of[g, mine, me.c, f] = normed(f)
        targets = [me.other_z()] + [me.at_x(d) for d in range(1, nx)] + [me.other_core()]
        for slot, device in enumerate(targets):
            for part in range(parts):
                copy = row_copy(g, mine, me.c, slot, part, device)
                copy.start()
                row_sends.append(copy)

    def spread(g, p, slot, part, across):
        row_wait(g, p, me.c, part)
        targets = [me.at_x(d) for d in range(1, nx)] if across else []
        targets += [me.other_core()]
        for m, device in enumerate(targets):
            copy = row_copy(g, p, me.c, slot + m, part, device)
            copy.start()
            row_sends.append(copy)

    def near_rows(g):
        for part in range(parts):
            spread(g, rest, nx + 1, part, True)

    def far_rows(g):
        slot = 2 * nx + 1
        for base in (me.zp * nx, (1 - me.zp) * nx):
            for d in range(1, nx):
                for part in range(parts):
                    spread(g, base + (me.x + d) % nx, slot, part, False)
                slot += 1
        for p in range(chips):
            for part in range(parts):
                row_wait(g, p, 1 - me.c, part)

    def core_part(g, f):
        return remote(xs.at[f], xr.at[f], xss.at[g, f], xsr.at[g, f], me.other_core())

    def x_part(g, f, s):
        return remote(
            ys.at[f, s - 1], yr.at[f, s - 1], yss.at[g, f, s - 1], ysr.at[g, f, s - 1], me.at_x(s)
        )

    def z_part(g, f):
        return remote(zs.at[f], zr.at[f], zss.at[g, f], zsr.at[g, f], me.other_z())

    order = [(0, 0)]
    for i in range(1, nz + 1):
        order += [(i, 0)] if i < nz else []
        order += [(i - 1, j) for j in range(1, ny)]

    def reduce_rows(g, s, hidden, early=(), paced=False):
        last = MATS - 1

        def begin(m):
            i, j = order[m]
            f = me.f_at(i, j)
            if j:
                arrived(s, last, f)
            elif i == 0:
                local_piece(s, last).wait()
            elif i not in early:
                forward(s, last, i)
            weight = weights[s][last, f]
            term = jnp.dot(hidden[1 - me.c], weight, preferred_element_type=jnp.float32)
            xs[f] = term.astype(jnp.bfloat16).reshape(chips, r, dn)
            core_part(g, f).start()
            term = jnp.dot(hidden[me.c], weight, preferred_element_type=jnp.float32)
            part_sum[m % 2] = term.reshape(chips, r, dn)

        def cross(m):
            f = me.f_at(*order[m])
            core_part(g, f).wait_recv()
            for h in range(PAIR):
                for d in range(1, nx):
                    p = h * nx + (me.x + d) % nx
                    total = part_sum[m % 2, p] + xr[f, p].astype(jnp.float32)
                    ys[f, d - 1, h] = total.astype(jnp.bfloat16)
            for d in range(1, nx):
                x_part(g, f, d).start()
            for h in range(PAIR):
                p = h * nx + me.x
                own[f, h] = part_sum[m % 2, p] + xr[f, p].astype(jnp.float32)

        def pass_on(m):
            f = me.f_at(*order[m])
            total = own[f, 1 - me.zp]
            for d in range(1, nx):
                x_part(g, f, d).wait_recv()
                total = total + yr[f, d - 1, 1 - me.zp].astype(jnp.float32)
            zs[f] = total.astype(jnp.bfloat16)
            z_part(g, f).start()

        for m in range(n + 3):
            if paced and 1 <= m <= n:
                cross(m - 1)
            if m < n:
                begin(m)
            if not paced and 1 <= m <= n:
                cross(m - 1)
            if m >= 3:
                pass_on(m - 3)

    def reduced(g, f):
        z_part(g, f).wait_recv()
        total = own[f, me.zp]
        for d in range(1, nx):
            total = total + yr[f, d - 1, me.zp].astype(jnp.float32)
        return total + zr[f].astype(jnp.float32)

    def drain(g):
        def one(f, carry):
            core_part(g, f).wait_send()
            for d in range(1, nx):
                x_part(g, f, d).wait_send()
            z_part(g, f).wait_send()
            return carry

        lax.fori_loop(0, n, one, 0)

    def project(g, s, k, c, to):
        acc[to] = jnp.zeros_like(acc[to])

        def feature(m, carry):
            rows = [rows_of[g, :, c, m * group + d].reshape(chips * r, dn) for d in range(group)]
            units = [weights[s][k, m * group + d] for d in range(group)]
            acc[to] += dot_nt(jnp.concatenate(rows, axis=1), jnp.concatenate(units, axis=1))
            return carry

        lax.fori_loop(0, n // group, feature, 0)

    def gate_rows(g, s):
        def side(c, carry):
            project(g, s, 0, c, c)
            return carry

        lax.fori_loop(0, CORES, side, 0)

    def hidden_rows(g, s, between=()):
        for c in (1 - me.c, me.c):
            project(g, s, 1, c, CORES)
            gate = acc[c]
            hid[c] = (gate * sigmoid(gate) * acc[CORES]).astype(jnp.bfloat16)
            forward_all(s, MATS - 1, between)
            between = ()

    def mix_rows(g, s):
        acc_m[...] = jnp.zeros_like(acc_m)
        length = nx * CORES * r

        def feature(f, carry):
            rows = rows_of[g, :, :, f].reshape(PAIR * length, dn)
            for k in range(MATS - 1):
                acc_m[k] += dot_nt(rows, weights[s][k, f])
            return carry

        lax.fori_loop(0, n, feature, 0)
        channels = taps.shape[1] // PAIR

        def mine_of(v):
            return jnp.where(me.zp == 0, v[:, :channels], v[:, channels:])

        tap = mine_of(taps[...].astype(jnp.float32))
        fall = mine_of(slope[...])
        count, size = gate_a.shape[0] // PAIR, gate_a.shape[1]
        for wide, gate in ((wide_a, gate_a), (wide_x, gate_x)):
            wide[...] = jnp.zeros_like(wide)
            for m in range(count):
                at = slice(m * size, (m + 1) * size)
                wide[at, at] = gate[me.zp * count + m].astype(jnp.float32)
        a, b = wide_a[...].astype(jnp.bfloat16), wide_x[...].astype(jnp.bfloat16)
        for q in range(PAIR):
            rows = pl.ds(q * length, length)
            lru = acc_m[0, rows].astype(jnp.bfloat16).astype(jnp.float32)
            gated = acc_m[1, rows].astype(jnp.bfloat16).astype(jnp.float32)
            conv = tap[0:1] * lru
            for k in range(1, tap.shape[0]):
                conv = conv + tap[k : k + 1] * shift_down(lru, k, 0.0)
            low = conv.astype(jnp.bfloat16)
            recall = sigmoid(jnp.dot(low, a, preferred_element_type=jnp.float32))
            admit = sigmoid(jnp.dot(low, b, preferred_element_type=jnp.float32))
            log_keep = -8.0 * recall * fall
            keep = jnp.exp(log_keep)
            grow = -jnp.tanh(log_keep) * (1.0 + keep * keep)
            state = jnp.sqrt(grow) * admit * low.astype(jnp.float32)
            step = 1
            while step < length:
                state = state + keep * shift_down(state, step, 0.0)
                keep = keep * shift_down(keep, step, 1.0)
                step *= 2
            inner = 0.7978845608028654 * (gated + 0.044715 * gated * gated * gated)
            mixed = state * (0.5 * gated * (1.0 + jnp.tanh(inner)))
            mixed = mixed.astype(jnp.bfloat16)
            for x in range(nx):
                for c in range(CORES):
                    at = (x * CORES + c) * r
                    hid_m[c, pl.ds((q * nx + x) * r, r)] = mixed[at : at + r]

    first = range(PAIR, nz, PAIR)
    second = range(PAIR + 1, nz, PAIR)

    def forward_all(s, k, which):
        for i in which:
            forward(s, k, i)

    def take_near(s, k):
        forward(s, k, 1)

    when_end((send_both, 0, 0))
    when_inner((send_near, 0, 0), (to_inner, 0, 0))
    send_own(0, 0)
    send_rows(0, lambda f: tokens[f].astype(jnp.float32), gain1)
    flip(0, 1)
    when_end((send_both, 0, 1), (send_both, 0, 2))
    when_inner((send_near, 0, 1), (to_inner, 0, 1), (to_end, 0, 0), (send_near, 0, 2))
    send_own(0, 1)
    for s in (1, 2):
        for k in range(MATS - 1):
            flip(s, k)
    take_near(0, 0)
    when_inner((relay, 0, 0), (to_end, 0, 1))
    near_rows(0)
    forward_all(0, 0, first)
    far_rows(0)
    when_inner((take_near, 0, 1), (relay, 0, 1), (to_inner, 0, 2), (to_end, 0, 2))
    forward_all(0, 0, second)
    when_end((take_near, 0, 1))
    forward_all(0, 1, first)
    collect(0, 0)
    when_end(*[(send_both, 1, k) for k in range(MATS)], (send_both, 2, 0), (send_both, 2, 1))
    gate_rows(0, 0)
    forward_all(0, 1, second)
    send_own(0, 2)
    take_near(0, 2)
    when_inner((relay, 0, 2))
    when_inner(*[(act, 1, k) for k in range(MATS) for act in (send_near, to_inner, to_end, relay)])
    collect(0, 1)
    when_inner(*[(take_near, 1, k) for k in range(MATS)])
    when_inner((send_near, 2, 0), (send_near, 2, 1), (to_inner, 2, 0), (to_inner, 2, 1))
    hidden_rows(0, 0)
    reduce_rows(0, 0, hid, [1], True)
    when_end(*[(take_near, 1, k) for k in range(MATS)])
    for k in range(MATS):
        send_own(1, k)
    send_own(2, 0)
    for f in range(n):
        res[f] = (tokens[f].astype(jnp.float32) + 0.5 * reduced(0, f)).astype(jnp.bfloat16)
    send_rows(1, lambda f: res[f].astype(jnp.float32), gainm)
    when_end((send_both, 2, 2))
    for k in range(MATS):
        forward_all(1, k, range(2, nz))
    when_end((take_near, 2, 0), (take_near, 2, 1))
    near_rows(1)
    when_inner((to_end, 2, 0), (take_near, 2, 0), (to_end, 2, 1), (take_near, 2, 1))
    when_inner((relay, 2, 0), (relay, 2, 1), (to_inner, 2, 2))
    when_inner((send_near, 2, 2))
    send_own(2, 1)
    far_rows(1)
    for k in range(MATS - 1):
        collect(1, k)
    mix_rows(1, 1)
    forward_all(2, 0, first)
    drain(0)
    reduce_rows(1, 1, hid_m, range(1, nz))
    forward_all(2, 1, first)
    for f in range(n):
        res[f] = (res[f].astype(jnp.float32) + reduced(1, f)).astype(jnp.bfloat16)
    send_rows(2, lambda f: res[f].astype(jnp.float32), gain2)
    forward_all(2, 0, second)
    near_rows(2)
    when_inner((to_end, 2, 2), (relay, 2, 2))
    when_inner((take_near, 2, 2))
    forward_all(2, 1, second)
    when_end((take_near, 2, 2))
    send_own(2, 2)
    far_rows(2)
    collect(2, 0)
    gate_rows(2, 2)
    collect(2, 1)
    hidden_rows(2, 2, first)
    drain(1)
    reduce_rows(2, 2, hid, [1, *first], True)
    for f in range(n):
        out[f] = (res[f].astype(jnp.float32) + 0.5 * reduced(2, f)).astype(jnp.bfloat16)

    for copy in row_sends:
        copy.wait_send()
    for s in range(3):
        for k in range(MATS):
            z_piece(s, k, 1).wait_send()
            for i in range(nz):
                for j in range(1, ny):
                    y_piece(s, k, i, j).wait_send()

    def finish_inner(s, k):
        for i in range(PAIR, nz):
            z_piece(s, k, i).wait_send()
            (relay_near if i % PAIR else relay_out)(s, k, i).wait_send()

    def finish_end(s, k):
        relay_in(s, k).wait_send()

    when_inner(*[(finish_inner, s, k) for s in range(3) for k in range(MATS)])
    when_end(*[(finish_end, s, k) for s in range(3) for k in range(MATS)])

    drain(2)


def body(
    n,
    t,
    tokens,
    ffn1_gain,
    ffn1_gate,
    ffn1_up,
    ffn1_down,
    mix_gain,
    lru_in_weight,
    lru_gate_weight,
    conv_weight,
    gate_a_weight,
    gate_x_weight,
    decay_param,
    mix_out_weight,
    ffn2_gain,
    ffn2_gate,
    ffn2_up,
    ffn2_down,
):
    r, width = tokens.shape
    dn = width // n
    ny = math.isqrt(n // PAIR)
    nz, nx = n // ny, t // CORES
    chips = PAIR * nx
    parts = math.gcd(n, ROW_PARTS)
    hs = ffn1_gate.shape[1] // PAIR
    size = gate_a_weight.shape[1]
    extra = -gate_a_weight.shape[0] % PAIR
    if extra:
        lru_in_weight, lru_gate_weight, conv_weight = (
            jnp.pad(w, ((0, 0), (0, extra * size))) for w in (lru_in_weight, lru_gate_weight, conv_weight)
        )
        gate_a_weight, gate_x_weight = (
            jnp.pad(w, ((0, extra), (0, 0), (0, 0))) for w in (gate_a_weight, gate_x_weight)
        )
        decay_param = jnp.pad(decay_param, (0, extra * size))
        mix_out_weight = jnp.pad(mix_out_weight, ((0, extra * size), (0, 0)))
    cs = lru_in_weight.shape[1] // PAIR

    small = [
        tokens,
        ffn1_gain[None],
        mix_gain[None],
        ffn2_gain[None],
        conv_weight,
        gate_a_weight,
        gate_x_weight,
        jax.nn.softplus(-decay_param)[None],
    ]
    big = [
        ffn1_gate,
        ffn1_up,
        ffn1_down.reshape(PAIR, hs, dn),
        lru_in_weight,
        lru_gate_weight,
        mix_out_weight.reshape(PAIR, cs, dn),
        ffn2_gate,
        ffn2_up,
        ffn2_down.reshape(PAIR, hs, dn),
    ]
    bf16, f32 = jnp.bfloat16, jnp.float32
    sem = pltpu.SemaphoreType.DMA
    scratch = [
        pltpu.VMEM((MATS, n, hs, dn), bf16),
        pltpu.VMEM((MATS, n, cs, dn), bf16),
        pltpu.VMEM((MATS, n, hs, dn), bf16),
        pltpu.VMEM((MATS, hs, dn), bf16),
        pltpu.VMEM((MATS, cs, dn), bf16),
        pltpu.VMEM((MATS, hs, dn), bf16),
        pltpu.VMEM((3, chips, CORES, n, r, dn), bf16),
        pltpu.VMEM((n, chips, r, dn), bf16),
        pltpu.VMEM((n, chips, r, dn), bf16),
        pltpu.VMEM((n, nx - 1, PAIR, r, dn), bf16),
        pltpu.VMEM((n, nx - 1, PAIR, r, dn), bf16),
        pltpu.VMEM((n, r, dn), bf16),
        pltpu.VMEM((n, r, dn), bf16),
        pltpu.VMEM((n, PAIR, r, dn), f32),
        pltpu.VMEM((2, chips, r, dn), f32),
        pltpu.VMEM((CORES, chips * r, hs), bf16),
        pltpu.VMEM((CORES + 1, chips * r, hs), f32),
        pltpu.VMEM((CORES, chips * r, cs), bf16),
        pltpu.VMEM((MATS - 1, CORES * chips * r, cs), f32),
        pltpu.VMEM((n, r, dn), bf16),
        pltpu.VMEM((n, r, dn), bf16),
        *[pltpu.VMEM((MATS - 1, dn, PAIR * u), bf16) for u in (hs, cs, hs)],
        *[pltpu.VMEM((MATS - 1, PAIR, u, dn), bf16) for u in (hs, cs, hs)],
        pltpu.VMEM((cs, cs), f32),
        pltpu.VMEM((cs, cs), f32),
        sem((3, MATS, n)),
        sem((3, MATS)),
        sem((3, MATS, 2 * nz)),
        sem((3, MATS, nz, ny)),
        sem((3, MATS)),
        sem((3, chips, CORES, parts)),
        sem((3, 4 * nx, parts)),
        sem((3, n)),
        sem((3, n)),
        sem((3, n, nx - 1)),
        sem((3, n, nx - 1)),
        sem((3, n)),
        sem((3, n)),
        sem((3, MATS)),
    ]
    vmem = pl.BlockSpec(memory_space=pltpu.VMEM)
    hbm = pl.BlockSpec(memory_space=pl.ANY)
    result = pl.pallas_call(
        functools.partial(layer_kernel, n, t),
        out_shape=jax.ShapeDtypeStruct((n, r, dn), bf16),
        in_specs=[vmem] * len(small) + [hbm] * len(big),
        out_specs=vmem,
        scratch_shapes=scratch,
        compiler_params=pltpu.CompilerParams(
            collective_id=0, has_side_effects=True, vmem_limit_bytes=66_000_000
        ),
    )(*small, *big)
    return result.transpose(1, 0, 2).reshape(r, width)


def solution(mesh):
    n, t = mesh.shape["fs"], mesh.shape["tp"]
    in_specs = (
        P(("fs", "tp"), None),
        P(),
        P("fs", "tp"),
        P("fs", "tp"),
        P("tp", "fs"),
        P(),
        P("fs", "tp"),
        P("fs", "tp"),
        P(None, "tp"),
        P("tp", None, None),
        P("tp", None, None),
        P("tp"),
        P("tp", "fs"),
        P(),
        P("fs", "tp"),
        P("fs", "tp"),
        P("tp", "fs"),
    )

    def run(*args):
        return body(n, t, *args)

    return jax.shard_map(
        run, mesh=mesh, in_specs=in_specs, out_specs=P(("fs", "tp"), None), check_vma=False
    )
```
